32 devices in a mesh: kv: 8 (over z, core), tp: 4 (over y, x).
Axes of the slice: x: 2, y: 2, z: 4, core: 2. Of those that a mesh axis runs over, the one named last changes fastest.
Arguments:
- tokens: bfloat16 [16, 2048], P(None, 'kv'), may hold values from -8 to 8
- lengths: int32 [16], replicated, may hold values from 1 to 3072, 12288 in all
- latent_cache: bfloat16 [16, 3072, 256], P(None, ('kv', 'tp')), may hold values from -10 to 10
- rope_cache: bfloat16 [16, 3072, 32], P(None, ('kv', 'tp')), may hold values from -2000 to 2000
- gain_in: bfloat16 [2048], P('kv'), may hold values from 0.099609375 to 1.8984375
- w_down_q: bfloat16 [2048, 512], P('kv'), may hold values from -0.125 to 0.125
- w_down_kv: bfloat16 [2048, 256], P('kv'), may hold values from -0.125 to 0.125
- w_rope_key: bfloat16 [2048, 32], P('kv'), may hold values from -0.125 to 0.125
- gain_q: bfloat16 [512], replicated, may hold values from 0.099609375 to 1.8984375
- w_up_qn: bfloat16 [512, 16, 64], replicated, may hold values from -0.25 to 0.25
- w_up_qr: bfloat16 [512, 16, 32], replicated, may hold values from -0.25 to 0.25
- gain_kv: bfloat16 [256], replicated, may hold values from 0.099609375 to 1.8984375
- w_key_up: bfloat16 [256, 16, 64], replicated, may hold values from -0.375 to 0.375
- w_value_up: bfloat16 [256, 16, 64], replicated, may hold values from -0.375 to 0.375
- w_attn_out: bfloat16 [16, 64, 2048], P('tp', None, 'kv'), may hold values from -0.1875 to 0.1875
- gain_mid: bfloat16 [2048], P('kv'), may hold values from 0.099609375 to 1.8984375
- w_ff_in: bfloat16 [2048, 8192], P('kv', 'tp'), may hold values from -0.125 to 0.125
- w_ff_out: bfloat16 [8192, 2048], P('tp', 'kv'), may hold values from -0.0625 to 0.0625
Outputs:
- mixed: bfloat16 [16, 2048], P(None, 'kv')
- new_latent: bfloat16 [16, 256], replicated
- new_rope_key: bfloat16 [16, 32], replicated
The draws below stay inside these ranges and needn't reach their ends.
Inputs may be any that keep to these rules, and one draw needn't show every extreme that they name: `lengths`: each sequence's live cache positions; one sequence fills the whole cache.
All inputs are finite; a program needn't handle non-finite values.
Results may differ from the reference program's by a relative error of at most 0.012.
Values sent between devices are 32-bit elements; how exact they have to be, the bound alone decides.
No kernel may reach another device: no remote copies, remote signals or barrier semaphores. Data moves between devices by JAX's collectives and lax.ppermute only.
A program may use at most 64 MiB of HBM per device.

```python
import math
import jax
import jax.numpy as jnp
import numpy as np
from jax import lax

D = 2048
H = 16
NOPE = 64
ROPE = 32
V = 64
QR = 512
KR = 256
FF = 8192
SEQS = 16
CACHE = 3072
N_KV = 8


def draw_tokens(key, part):
    first = jax.random.fold_in(key, 0)
    rising = 0.3 * 10.0 ** (jnp.arange(D, dtype=jnp.float32) / D)
    values = jax.random.normal(first, (SEQS, D), jnp.float32) * rising
    return jnp.clip(values, -8.0, 8.0).astype(jnp.bfloat16)


def draw_latent_cache(key, part):
    first = jax.random.fold_in(key, 0)
    values = jax.random.normal(first, (SEQS, CACHE, KR), jnp.float32) * 2.0
    return jnp.clip(values, -10.0, 10.0).astype(jnp.bfloat16)


def draw_rope_cache(key, part):
    first = jax.random.fold_in(key, 0)
    values = jax.random.normal(first, (SEQS, CACHE, ROPE), jnp.float32) * 2.0
    return jnp.clip(values, -2000.0, 2000.0).astype(jnp.bfloat16)


def levels(own_key, dims, cuts, low, top_value):
    factor_of, own = 1.0, jax.random.fold_in(own_key, 6)
    for dim, shards_of in cuts:
        draws = jnp.exp(jax.random.uniform(jax.random.fold_in(own, dim), (shards_of,), jnp.float32, low / len(cuts), top_value / len(cuts)))
        factor_of = factor_of * jnp.repeat(draws, dims[dim] // shards_of).reshape([-1 if axis == dim else 1 for axis in range(len(dims))])
    return factor_of


def profile(count, total, limit, slope):
    portions = [(1 << 20) // math.isqrt(rank ** slope) + 1 for rank in range(2, count + 1)]
    surplus, holding = total - limit - (count - 1), [1] * (count - 1)
    while surplus > 0:
        movable = [i for i in range(count - 1) if holding[i] < limit]
        whole, left = sum([portions[i] for i in movable]), surplus
        for i in movable:
            more = min(limit - holding[i], max(1, left * portions[i] // whole), surplus)
            holding[i] = holding[i] + more
            surplus = surplus - more
    return np.array([limit] + holding)


def uneven(key, amount, total, most, lean):
    if amount == 2:
        one = jax.random.randint(key, (), max(1, total - most), min(most, total - 1) + 1)
        return jnp.stack([one, total - one])
    sizes = jnp.asarray(profile(amount, total, most, lean), jnp.int32)
    pairs = (amount - 1) // 2
    donor, receiver = sizes[1:1 + 2 * pairs:2], sizes[2:2 + 2 * pairs:2]
    slack = jnp.minimum(donor - 1, most - receiver)
    moved = jax.random.randint(jax.random.fold_in(key, 1), (pairs,), 0, 1 << 20) % (slack + 1)
    sizes = sizes.at[1:1 + 2 * pairs:2].set(donor - moved).at[2:2 + 2 * pairs:2].set(receiver + moved)
    return sizes[jax.random.permutation(jax.random.fold_in(key, 2), amount)]


def scatter_about(rng, extent, deviation, most, cuts=(), kind=jnp.bfloat16):
    level = levels(rng, extent, cuts, -0.22, 0.18) if cuts else 1.0
    drawn = jax.random.normal(rng, extent, jnp.float32) * deviation * level
    return jnp.minimum(jnp.maximum(drawn, -most), most).astype(kind)


def setup_inputs(seed: int = 0) -> dict:
    streams_of = jax.random.split(jax.random.key(seed), 19)
    return {
        "tokens": draw_tokens(jax.random.fold_in(streams_of[18], 71), 0),
        "lengths": uneven(streams_of[1], SEQS, SEQS * CACHE // 4, CACHE, 2).astype(jnp.int32),
        "latent_cache": draw_latent_cache(jax.random.fold_in(streams_of[18], 71), 0),
        "rope_cache": draw_rope_cache(jax.random.fold_in(streams_of[18], 71), 0),
        "gain_in": jnp.clip(1.0 + 0.18 * jax.random.normal(streams_of[4], (D,), jnp.float32), 0.099609375, 1.8984375).astype(jnp.bfloat16),
        "w_down_q": scatter_about(streams_of[5], (D, QR), D ** -0.5, 0.125, ((0, 8),)),
        "w_down_kv": scatter_about(streams_of[6], (D, KR), D ** -0.5, 0.125, ((0, 8),)),
        "w_rope_key": scatter_about(streams_of[7], (D, ROPE), D ** -0.5, 0.125, ((0, 8),)),
        "gain_q": jnp.clip(1.0 + 0.18 * jax.random.normal(streams_of[8], (QR,), jnp.float32), 0.099609375, 1.8984375).astype(jnp.bfloat16),
        "w_up_qn": scatter_about(streams_of[9], (QR, H, NOPE), QR ** -0.5, 0.25),
        "w_up_qr": scatter_about(streams_of[10], (QR, H, ROPE), QR ** -0.5, 0.25),
        "gain_kv": jnp.clip(1.0 + 0.18 * jax.random.normal(streams_of[11], (KR,), jnp.float32), 0.099609375, 1.8984375).astype(jnp.bfloat16),
        "w_key_up": scatter_about(streams_of[12], (KR, H, NOPE), KR ** -0.5, 0.375),
        "w_value_up": scatter_about(streams_of[13], (KR, H, V), KR ** -0.5, 0.375),
        "w_attn_out": scatter_about(streams_of[14], (H, V, D), (H * V) ** -0.5, 0.1875, ((0, 4), (2, 8))),
        "gain_mid": jnp.clip(1.0 + 0.18 * jax.random.normal(streams_of[15], (D,), jnp.float32), 0.099609375, 1.8984375).astype(jnp.bfloat16),
        "w_ff_in": scatter_about(streams_of[16], (D, FF), D ** -0.5, 0.125, ((0, 8), (1, 4))),
        "w_ff_out": scatter_about(streams_of[17], (FF, D), FF ** -0.5, 0.0625, ((0, 4), (1, 8))),
    }


EPS = 1e-06

def rotate(values, positions):
    half = values.shape[-1] // 2
    inverse = 10000.0 ** (-jnp.arange(half, dtype=jnp.float32) / half)
    angle = positions.astype(jnp.float32)[:, None, None] * inverse[None, None, :]
    first = values[..., :half]
    second = values[..., half:]
    return jnp.concatenate([first * jnp.cos(angle) - second * jnp.sin(angle), second * jnp.cos(angle) + first * jnp.sin(angle)], axis=-1)

def rms_scaled(values, gain):
    return values * lax.rsqrt(lax.optimization_barrier(jnp.mean(values * values, axis=-1, keepdims=True)) + EPS) * gain.astype(jnp.float32)

def reference(tokens, lengths, latent_cache, rope_cache, gain_in, w_down_q, w_down_kv, w_rope_key, gain_q, w_up_qn, w_up_qr, gain_kv, w_key_up, w_value_up, w_attn_out, gain_mid, w_ff_in, w_ff_out):
    f32 = jnp.float32
    bf16 = jnp.bfloat16
    scale = (NOPE + ROPE) ** (-0.5)
    resid = tokens.astype(f32)
    scaled_in = (resid * gain_in.astype(f32)).astype(bf16)
    inv_in = lax.rsqrt(lax.optimization_barrier(jnp.mean(resid * resid, axis=1, keepdims=True)) + EPS)
    sum_q = jnp.dot(scaled_in, w_down_q, preferred_element_type=f32)
    sum_kv = jnp.dot(scaled_in, w_down_kv, preferred_element_type=f32)
    sum_rope = jnp.dot(scaled_in, w_rope_key, preferred_element_type=f32)
    query_latent = rms_scaled(inv_in * sum_q, gain_q).astype(bf16)
    new_latent = rms_scaled(inv_in * sum_kv, gain_kv).astype(bf16)
    new_rope_key = rotate((inv_in * sum_rope)[:, None, :], lengths)[:, 0, :].astype(bf16)
    query_nope = jnp.einsum('bc,chd->bhd', query_latent.astype(f32), w_up_qn.astype(f32)).astype(bf16)
    query_rope = rotate(jnp.einsum('bc,chr->bhr', query_latent.astype(f32), w_up_qr.astype(f32)), lengths).astype(bf16)
    query_cache = jnp.einsum('bhd,khd->bhk', query_nope.astype(f32), w_key_up.astype(f32)).astype(bf16)
    self_score = (jnp.einsum('bhk,bk->bh', query_cache.astype(f32), new_latent.astype(f32)) + jnp.einsum('bhr,br->bh', query_rope.astype(f32), new_rope_key.astype(f32))) * scale
    span = CACHE // N_KV
    latent_blocks = latent_cache.reshape(SEQS, N_KV, span, KR).swapaxes(0, 1)
    rope_blocks = rope_cache.reshape(SEQS, N_KV, span, ROPE).swapaxes(0, 1)

    def block_scores(args):
        latent_block, rope_block, index = args
        scores = (jnp.einsum('bhk,blk->bhl', query_cache.astype(f32), latent_block.astype(f32)) + jnp.einsum('bhr,blr->bhl', query_rope.astype(f32), rope_block.astype(f32))) * scale
        positions = index * span + jnp.arange(span, dtype=jnp.int32)
        live = positions[None, :] < lengths[:, None]
        return (jnp.where(live[:, None, :], scores, -1e+30), live)
    scores, lives = lax.map(block_scores, (latent_blocks, rope_blocks, jnp.arange(N_KV, dtype=jnp.int32)))
    top = jnp.maximum(lax.optimization_barrier(jnp.max(scores, axis=(0, 3))), self_score)
    weights = jnp.where(lives[:, :, None, :], jnp.exp(scores - top[None, :, :, None]), 0.0)
    self_weight = jnp.exp(self_score - top)
    total = lax.optimization_barrier(jnp.sum(weights, axis=(0, 3))) + self_weight

    def add_block(acc, args):
        weight_block, latent_block = args
        term = jnp.einsum('bhl,blk->bhk', weight_block.astype(bf16).astype(f32), latent_block.astype(f32))
        return (acc + term, None)
    start = self_weight.astype(bf16).astype(f32)[:, :, None] * new_latent.astype(f32)[:, None, :]
    acc, _ = lax.scan(add_block, start, (weights, latent_blocks))
    expanded = jnp.einsum('bhk,khv->bhv', acc, w_value_up.astype(f32), precision=lax.Precision.HIGHEST)
    head_out = (expanded / total[:, :, None]).astype(bf16)
    resid_mid = resid + jnp.einsum('bhv,hvd->bd', head_out.astype(f32), w_attn_out.astype(f32))
    scaled_mid = (resid_mid * gain_mid.astype(f32)).astype(bf16)
    inv_mid = lax.rsqrt(lax.optimization_barrier(jnp.mean(resid_mid * resid_mid, axis=1, keepdims=True)) + EPS)
    hidden = jnp.square(jax.nn.relu(inv_mid * jnp.dot(scaled_mid, w_ff_in, preferred_element_type=f32))).astype(bf16)
    mixed = (resid_mid + jnp.dot(hidden, w_ff_out, preferred_element_type=f32)).astype(bf16)
    return (mixed, new_latent, new_rope_key)
```

```python
import jax
import jax.numpy as jnp
from jax import lax
from jax.sharding import PartitionSpec as P

D = 2048
NOPE = 64
ROPE = 32
EPS = 1e-06


def swap(value, axis, bit):
    size = lax.axis_size(axis)
    return lax.ppermute(value, axis, [(j, j ^ bit) for j in range(size)])


def bits(axis):
    size = lax.axis_size(axis)
    found = [1 << i for i in range(size.bit_length() - 1)]
    assert 1 << len(found) == size
    return found


def summed(value, axis, skip=()):
    for bit in bits(axis):
        if bit not in skip:
            value = value + swap(value, axis, bit)
    return value


def my_half(value, dim, axis, bit):
    half = value.shape[dim] // 2
    mine = (lax.axis_index(axis) & bit) // bit
    keep = lax.dynamic_slice_in_dim(value, mine * half, half, dim)
    give = lax.dynamic_slice_in_dim(value, (1 - mine) * half, half, dim)
    return keep, give


def rotate(values, positions):
    half = values.shape[-1] // 2
    inverse = 10000.0 ** (-jnp.arange(half, dtype=jnp.float32) / half)
    angle = positions.astype(jnp.float32)[:, None, None] * inverse[None, None, :]
    first = values[..., :half]
    second = values[..., half:]
    return jnp.concatenate(
        [
            first * jnp.cos(angle) - second * jnp.sin(angle),
            second * jnp.cos(angle) + first * jnp.sin(angle),
        ],
        axis=-1,
    )


def rms_scaled(values, gain):
    return (
        values
        * lax.rsqrt(jnp.mean(values * values, axis=-1, keepdims=True) + EPS)
        * gain.astype(jnp.float32)
    )


def merged(one, two):
    top_one, top_two = one[..., -1:], two[..., -1:]
    top = jnp.maximum(top_one, top_two)
    body = one[..., :-1] * jnp.exp(top_one - top) + two[..., :-1] * jnp.exp(top_two - top)
    return jnp.concatenate([body, top], axis=-1)


def per_device(
    tokens,
    lengths,
    latent_cache,
    rope_cache,
    gain_in,
    w_down_q,
    w_down_kv,
    w_rope_key,
    gain_q,
    w_up_qn,
    w_up_qr,
    gain_kv,
    w_key_up,
    w_value_up,
    w_attn_out,
    gain_mid,
    w_ff_in,
    w_ff_out,
):
    f32 = jnp.float32
    bf16 = jnp.bfloat16
    scale = (NOPE + ROPE) ** (-0.5)
    resid = tokens.astype(f32)
    scaled_in = (resid * gain_in.astype(f32)).astype(bf16)
    part_q = jnp.dot(scaled_in, w_down_q, preferred_element_type=f32)
    part_kv = jnp.dot(scaled_in, w_down_kv, preferred_element_type=f32)
    part_rope = jnp.dot(scaled_in, w_rope_key, preferred_element_type=f32)
    square_in = jnp.sum(resid * resid, axis=1, keepdims=True)
    sums = summed(jnp.concatenate([part_q, part_kv, part_rope, square_in], axis=1), "kv")
    ends = [w_down_q.shape[1], w_down_q.shape[1] + w_down_kv.shape[1]]
    ends.append(ends[1] + w_rope_key.shape[1])
    sum_q, sum_kv, sum_rope, total_in = jnp.split(sums, ends, axis=1)
    inv_in = lax.rsqrt(total_in / D + EPS)
    query_latent = rms_scaled(inv_in * sum_q, gain_q).astype(bf16)
    new_latent = rms_scaled(inv_in * sum_kv, gain_kv).astype(bf16)
    new_rope_key = rotate((inv_in * sum_rope)[:, None, :], lengths)[:, 0, :].astype(bf16)
    query_nope = jnp.einsum(
        "bc,chd->bhd", query_latent, w_up_qn, preferred_element_type=f32
    ).astype(bf16)
    query_rope = rotate(
        jnp.einsum("bc,chr->bhr", query_latent, w_up_qr, preferred_element_type=f32), lengths
    ).astype(bf16)
    query_cache = jnp.einsum(
        "bhd,khd->bhk", query_nope, w_key_up, preferred_element_type=f32
    ).astype(bf16)
    rows = latent_cache.shape[1]
    positions = lax.axis_index(("kv", "tp")) * rows + jnp.arange(rows, dtype=jnp.int32)
    live = (positions[None, :] < lengths[:, None])[:, None, :]
    scores = (
        jnp.einsum("bhk,blk->bhl", query_cache, latent_cache, preferred_element_type=f32)
        + jnp.einsum("bhr,blr->bhl", query_rope, rope_cache, preferred_element_type=f32)
    ) * scale
    scores = jnp.where(live, scores, -1e30)
    top = jnp.max(scores, axis=2)
    weights = jnp.where(live, jnp.exp(scores - top[:, :, None]), 0.0)
    total = jnp.sum(weights, axis=2)
    acc = jnp.einsum("bhl,blk->bhk", weights.astype(bf16), latent_cache, preferred_element_type=f32)
    expanded = jnp.einsum(
        "bhk,khv->hbv", acc, w_value_up.astype(f32), precision=lax.Precision.HIGHEST
    )
    part = jnp.concatenate([expanded, total.T[:, :, None], top.T[:, :, None]], axis=2)
    for bit in reversed(bits("tp")):
        keep, give = my_half(part, 0, "tp", bit)
        part = merged(keep, swap(give, "tp", bit))
    for bit in bits("kv"):
        part = merged(part, swap(part, "kv", bit))
    heads_dev = w_attn_out.shape[0]
    first_head = lax.axis_index("tp") * heads_dev
    own_value_up = lax.dynamic_slice_in_dim(w_value_up, first_head, heads_dev, 1)
    own_cache_q = lax.dynamic_slice_in_dim(query_cache, first_head, heads_dev, 1)
    own_rope_q = lax.dynamic_slice_in_dim(query_rope, first_head, heads_dev, 1)
    self_score = (
        jnp.einsum("bhk,bk->hb", own_cache_q, new_latent, preferred_element_type=f32)
        + jnp.einsum("bhr,br->hb", own_rope_q, new_rope_key, preferred_element_type=f32)
    ) * scale
    self_value = jnp.einsum("bk,khv->hbv", new_latent, own_value_up, preferred_element_type=f32)
    top, total, expanded = part[..., -1], part[..., -2], part[..., :-2]
    joined = jnp.maximum(top, self_score)
    fade = jnp.exp(top - joined)
    self_weight = jnp.exp(self_score - joined)
    total = total * fade + self_weight
    expanded = (
        expanded * fade[..., None] + self_weight.astype(bf16).astype(f32)[..., None] * self_value
    )
    head_out = (expanded / total[..., None]).astype(bf16)
    attn_part = jnp.einsum("hbv,hvd->bd", head_out, w_attn_out, preferred_element_type=f32)
    resid_mid = resid + summed(attn_part, "tp")
    scaled_mid = (resid_mid * gain_mid.astype(f32)).astype(bf16)
    hidden_part = jnp.dot(scaled_mid, w_ff_in, preferred_element_type=f32)
    square_mid = jnp.sum(resid_mid * resid_mid, axis=1, keepdims=True)
    keep, give = my_half(hidden_part, 1, "kv", 1)
    keep = jnp.concatenate([keep, square_mid], axis=1)
    give = jnp.concatenate([give, square_mid], axis=1)
    sums = summed(keep + swap(give, "kv", 1), "kv", skip=(1,))
    other = swap(sums, "kv", 1)
    low = (lax.axis_index("kv") & 1) == 0
    inv_mid = lax.rsqrt(sums[:, -1:] / D + EPS)
    sums = jnp.concatenate(
        [jnp.where(low, sums, other)[:, :-1], jnp.where(low, other, sums)[:, :-1]], axis=1
    )
    hidden = jnp.square(jax.nn.relu(inv_mid * sums)).astype(bf16)
    out_part = jnp.dot(hidden, w_ff_out, preferred_element_type=f32)
    mixed = (resid_mid + summed(out_part, "tp")).astype(bf16)
    return (mixed, new_latent, new_rope_key)


def solution(mesh):
    return jax.shard_map(
        per_device,
        mesh=mesh,
        in_specs=(
            P(None, "kv"),
            P(),
            P(None, ("kv", "tp"), None),
            P(None, ("kv", "tp"), None),
            P("kv"),
            P("kv", None),
            P("kv", None),
            P("kv", None),
            P(),
            P(),
            P(),
            P(),
            P(),
            P(),
            P("tp", None, "kv"),
            P("kv"),
            P("kv", "tp"),
            P("tp", "kv"),
        ),
        out_specs=(P(None, "kv"), P(), P()),
        check_vma=False,
    )
```

```python
import functools

import jax
import jax.numpy as jnp
import numpy as np
from jax import lax
from jax.experimental import pallas as pl
from jax.experimental.pallas import tpu as pltpu
from jax.sharding import PartitionSpec as P

D = 2048
EPS = 1e-06
LANES = 128
MXU = 256
f32 = jnp.float32
bf16 = jnp.bfloat16
BOTH = ("kv", "tp")


def swap(value, kv_mask, tp_mask=0):
    n_kv, n_tp = lax.axis_size("kv"), lax.axis_size("tp")
    pairs = [
        (k * n_tp + t, (k ^ kv_mask) * n_tp + (t ^ tp_mask)) for k in range(n_kv) for t in range(n_tp)
    ]
    return lax.ppermute(value, BOTH, pairs)


def higher_bits(axis, first):
    size = lax.axis_size(axis)
    assert size & (size - 1) == 0
    return [1 << i for i in range(first, size.bit_length() - 1)]


def parity():
    ones = 0
    for axis in BOTH:
        index = lax.axis_index(axis)
        for i in range(lax.axis_size(axis).bit_length() - 1):
            ones = ones ^ ((index >> i) & 1)
    return ones


def call(kernel, outs, *args, scratch=(), far=()):
    near = pl.BlockSpec(memory_space=pltpu.VMEM)
    return pl.pallas_call(
        kernel,
        out_shape=[pltpu.VMEM(s, t) for s, t in outs],
        in_specs=[near] * len(args) + [pl.BlockSpec(memory_space=pltpu.HBM)] * len(far),
        out_specs=[near] * len(outs),
        scratch_shapes=list(scratch),
        compiler_params=pltpu.CompilerParams(vmem_limit_bytes=16 * 1024 * 1024),
    )(
        *[pltpu.with_memory_space_constraint(a, pltpu.VMEM) for a in args],
        *[pltpu.with_memory_space_constraint(a, pltpu.HBM) for a in far],
    )


def fetched(sources, targets, semaphores):
    copies = [
        pltpu.make_async_copy(source, target, semaphores.at[i])
        for i, (source, target) in enumerate(zip(sources, targets, strict=True))
    ]
    for copy in copies:
        copy.start()
    return copies


def dot(a, b):
    return jnp.dot(a, b, preferred_element_type=f32)


def dot_t(a, b):
    return lax.dot_general(a, b, (((1,), (1,)), ((), ())), preferred_element_type=f32)


def lane(shape):
    return lax.broadcasted_iota(jnp.int32, shape, len(shape) - 1)


def down_kernel(*refs):
    far, (out, send), near, sems = refs[:6], refs[6:8], refs[8:14], refs[14]
    copies = fetched(far, near, sems)
    tokens, gain, w_q, w_kv, w_rope, w_out = near
    copies[0].wait()
    copies[1].wait()
    resid = tokens[...].astype(f32)
    scaled = (resid * gain[...].astype(f32)[None, :]).astype(bf16)
    q, kv = w_q.shape[1], w_kv.shape[1]
    copies[2].wait()
    out[:, :q] = dot(scaled, w_q[...])
    copies[3].wait()
    out[:, q : q + kv] = dot(scaled, w_kv[...])
    copies[4].wait()
    tail = dot_t(scaled, w_rope[...])
    square = jnp.sum(resid * resid, axis=1, keepdims=True)
    rest = LANES - tail.shape[1]
    out[:, q + kv :] = jnp.concatenate(
        [tail, jnp.broadcast_to(square, (tail.shape[0], rest))], axis=1
    )
    copies[5].wait()
    send[...] = w_out[...].astype(f32)


def fetch_kernel(*refs):
    count = (len(refs) - 2) // 2
    for copy in fetched(refs[1 : 1 + count], refs[1 + count : -1], refs[-1]):
        copy.wait()


def normed(values, gain):
    return values * lax.rsqrt(jnp.mean(values * values, axis=-1, keepdims=True) + EPS) * gain


def gathered(ref, start, count, stride):
    return jnp.concatenate(
        [ref[c, pl.ds(start, count, stride=stride), :] for c in range(ref.shape[0])], axis=1
    )


def rotate(values, cosine, sine, size):
    low = lane(values.shape) % size < size // 2
    other = jnp.where(
        low, pltpu.roll(values, LANES - size // 2, 1), pltpu.roll(values, size // 2, 1)
    )
    return values * cosine + other * sine


def attend_kernel(
    heads,
    sums,
    gain_q,
    gain_kv,
    cosine,
    sine,
    angle,
    w_nope,
    w_rope,
    w_key,
    w_value,
    latent,
    rope,
    new_latent,
    new_rope,
    queries,
    keep,
    give,
    accs,
    scored,
):
    n_seq, rows, kr = latent.shape
    rp = rope.shape[1]
    qr = gain_q.shape[0]
    nope = w_key.shape[0] // heads
    vs = w_value.shape[0] // heads
    scale = (nope + rp) ** (-0.5)
    tail = sums[:, qr + kr :]
    inv_in = lax.rsqrt(tail[:, LANES - 1 :] / D + EPS)
    query_latent = normed(inv_in * sums[:, :qr], gain_q[...].astype(f32)[None, :]).astype(bf16)
    new_latent[...] = normed(inv_in * sums[:, qr : qr + kr], gain_kv[...].astype(f32)[None, :]).astype(bf16)
    rotated = rotate(inv_in * tail, cosine[...], sine[...], rp)
    new_rope[...] = rotated[:, :rp].astype(bf16)
    up = dot_t(query_latent, w_nope[...])
    per = MXU // nope
    for g in range(heads // per):
        part = up[:, g * MXU : (g + 1) * MXU]
        block = lane(part.shape) // nope
        lhs = jnp.concatenate([jnp.where(block == i, part, 0.0) for i in range(per)], axis=0)
        wide = dot(lhs.astype(bf16), w_key[g * MXU : (g + 1) * MXU, :])
        for c in range(kr // LANES):
            queries[c, g * per * n_seq : (g + 1) * per * n_seq, :] = wide[
                :, c * LANES : (c + 1) * LANES
            ]
    turned = dot_t(query_latent, w_rope[...])
    rotated = jnp.concatenate(
        [
            rotate(turned[:, i : i + LANES], cosine[...], sine[...], rp)
            for i in range(0, heads * rp, LANES)
        ],
        axis=1,
    )
    for h in range(heads):
        queries[kr // LANES, h * n_seq : (h + 1) * n_seq, :rp] = rotated[:, h * rp : (h + 1) * rp]
    first = (lax.axis_index("kv") * lax.axis_size("tp") + lax.axis_index("tp")) * rows
    position = (first + lane((heads, rows))).astype(f32)
    low = lane((heads, LANES)) < LANES // 2
    for s in range(n_seq):
        own = gathered(queries, s, heads, n_seq).astype(bf16)
        scored[s] = (
            dot_t(own[:, :kr], latent[s]) + dot(own[:, kr : kr + rp], rope[s])
        ) * scale
    for s in range(n_seq):
        live = position < angle[s : s + 1, 0:1]
        scores = jnp.where(live, scored[s], -1e30)
        top = jnp.max(scores, axis=1, keepdims=True)
        weights = jnp.where(live, jnp.exp(scores - top), 0.0)
        total = jnp.sum(weights, axis=1, keepdims=True)
        scored[s] = weights
        accs[kr // LANES, s * heads : (s + 1) * heads, :] = jnp.where(low, top, total)
    for s in range(n_seq):
        acc = dot(scored[s].astype(bf16), latent[s])
        for c in range(kr // LANES):
            accs[c, s * heads : (s + 1) * heads, :] = acc[:, c * LANES : (c + 1) * LANES]
    per = MXU // vs
    groups = []
    for g in range(heads // per):
        acc = jnp.concatenate(
            [gathered(accs, g * per + i, n_seq, heads)[:, :kr] for i in range(per)], axis=0
        )
        coarse = acc.astype(bf16)
        fine = (acc - coarse.astype(f32)).astype(bf16)
        wide = dot_t(
            jnp.concatenate([coarse, fine], axis=0), w_value[g * MXU : (g + 1) * MXU, :]
        )
        wide = wide[: per * n_seq] + wide[per * n_seq :]
        block = lane((n_seq, MXU)) // vs
        groups.append(
            sum(
                jnp.where(block == i, wide[i * n_seq : (i + 1) * n_seq, :], 0.0)
                for i in range(per)
            )
        )
    in_half = heads // 2
    place = lane((n_seq, LANES)) % (LANES // 2)
    halves = []
    for half in range(2):
        stats = jnp.zeros((n_seq, LANES), f32)
        for i in range(in_half):
            each = accs[kr // LANES, pl.ds(half * in_half + i, n_seq, stride=heads), :]
            stats = jnp.where(place == i, each, stats)
        mine = groups[half * len(groups) // 2 : (half + 1) * len(groups) // 2]
        halves.append(jnp.concatenate(mine + [stats], axis=1))
    upper = parity() == 1
    keep[...] = jnp.where(upper, halves[1], halves[0])
    give[...] = jnp.where(upper, halves[0], halves[1])


def spread(factor, heads, width):
    n_seq = factor.shape[0]
    per = LANES // width
    block = lane((n_seq, LANES)) // width
    tiles = []
    for g in range(heads // per):
        tile = jnp.broadcast_to(factor[:, g * per : g * per + 1], (n_seq, LANES))
        for i in range(1, per):
            tile = jnp.where(block == i, factor[:, g * per + i : g * per + i + 1], tile)
        tiles.append(tile)
    return jnp.concatenate(tiles, axis=1)


def merge_kernel(in_half, one, two, out):
    body = one.shape[1] - LANES
    low = lane((one.shape[0], LANES)) < LANES // 2
    stats_one, stats_two = one[:, body:], two[:, body:]
    top = jnp.where(low, jnp.maximum(stats_one, stats_two), 0.0)
    fade_one = jnp.exp(jnp.where(low, stats_one - top, 0.0))
    fade_two = jnp.exp(jnp.where(low, stats_two - top, 0.0))
    total = stats_one * pltpu.roll(fade_one, LANES // 2, 1) + stats_two * pltpu.roll(
        fade_two, LANES // 2, 1
    )
    out[:, body:] = jnp.where(low, top, total)
    width = body // in_half
    out[:, :body] = one[:, :body] * spread(fade_one, in_half, width) + two[:, :body] * spread(
        fade_two, in_half, width
    )


def self_kernel(heads, nope, new_latent, new_rope, queries, w_value, scores, values):
    n_seq, kr = new_latent.shape
    rp = new_rope.shape[1]
    scale = (nope + rp) ** (-0.5)
    key, key_rope = new_latent[...].astype(f32), new_rope[...].astype(f32)
    in_half = heads // 2
    where = lane((n_seq, LANES))
    for half in range(2):
        tile = jnp.zeros((n_seq, LANES), f32)
        for i in range(in_half):
            h = half * in_half + i
            query = jnp.concatenate(
                [queries[c, h * n_seq : (h + 1) * n_seq, :] for c in range(queries.shape[0])],
                axis=1,
            )
            query = query.astype(bf16).astype(f32)
            score = jnp.sum(query[:, :kr] * key, axis=1, keepdims=True) + jnp.sum(
                query[:, kr : kr + rp] * key_rope, axis=1, keepdims=True
            )
            tile = jnp.where(where == i, score * scale, tile)
        scores[half] = tile
    values[...] = dot_t(new_latent[...], w_value[...])


def middle_kernel(
    heads, *refs
):
    (own, other, self_scores, self_values, tokens, gain, w_in), refs = refs[:7], refs[7:]
    n_tp = lax.axis_size("tp")
    w_outs, (mid, keep, give, outs) = refs[:n_tp], refs[n_tp:]
    n_seq = tokens.shape[0]
    in_half = heads // 2
    body = own.shape[1] - LANES
    width = body // in_half
    low = lane((n_seq, LANES)) < LANES // 2
    upper = parity() == 1
    group = w_outs[0].shape[0]
    for half in range(2):
        mine = upper if half == 1 else jnp.logical_not(upper)
        part = jnp.where(mine, own[...], other[...])
        stats = part[:, body:]
        scores = self_scores[half]
        top = jnp.where(low, jnp.maximum(stats, scores), 0.0)
        fade = jnp.exp(jnp.where(low, stats - top, 0.0))
        weight = jnp.exp(jnp.where(low, scores - top, 0.0))
        total = pltpu.roll(stats, LANES // 2, 1) * fade + weight
        total = jnp.where(low, total, 1.0)
        values = self_values[:, half * body : (half + 1) * body]
        joined = part[:, :body] * spread(fade / total, in_half, width) + values * spread(
            weight.astype(bf16).astype(f32) / total, in_half, width
        )
        joined = joined.astype(bf16)
        for g in range(body // group):
            outs[half * (body // group) + g] = joined[:, g * group : (g + 1) * group]
    me = lax.axis_index("tp")
    attn = dot(outs[me], w_outs[0][...].astype(bf16))
    for m in range(1, n_tp):
        attn += dot(outs[jnp.bitwise_xor(me, m)], w_outs[m][...].astype(bf16))
    resid_mid = tokens[...].astype(f32) + attn
    mid[...] = resid_mid
    scaled = (resid_mid * gain[...].astype(f32)[None, :]).astype(bf16)
    square = jnp.broadcast_to(jnp.sum(resid_mid * resid_mid, axis=1, keepdims=True), (n_seq, LANES))
    hidden = dot(scaled, w_in[...])
    half = hidden.shape[1] // 2
    keep[:, :half] = jnp.where(upper, hidden[:, half:], hidden[:, :half])
    give[:, :half] = jnp.where(upper, hidden[:, :half], hidden[:, half:])
    keep[:, half:] = square
    give[:, half:] = square


def last_kernel(own, other, w_out, out):
    half = own.shape[1] - LANES
    inv_mid = lax.rsqrt(own[:, half : half + 1] / D + EPS)
    mine = parity()
    total = None
    for part, place in ((own, mine), (other, 1 - mine)):
        hidden = jnp.square(jax.nn.relu(inv_mid * part[:, :half])).astype(bf16)
        begin = pl.multiple_of(place * half, half)
        term = dot(hidden, w_out[pl.ds(begin, half), :])
        total = term if total is None else total + term
    out[...] = total


def per_device(
    tokens,
    lengths,
    latent_cache,
    rope_cache,
    gain_in,
    w_down_q,
    w_down_kv,
    w_rope_key,
    gain_q,
    w_up_qn,
    w_up_qr,
    gain_kv,
    w_key_up,
    w_value_up,
    w_attn_out,
    gain_mid,
    w_ff_in,
    w_ff_out,
):
    n_seq = tokens.shape[0]
    qr, heads, nope = w_up_qn.shape
    rp = w_up_qr.shape[2]
    kr, _, vs = w_value_up.shape
    d_dev = tokens.shape[1]
    w_nope = w_up_qn.transpose(1, 2, 0).reshape(heads * nope, qr)
    w_rope = w_up_qr.transpose(1, 2, 0).reshape(heads * rp, qr)
    w_key = w_key_up.transpose(1, 2, 0).reshape(heads * nope, kr)
    w_value = w_value_up.transpose(1, 2, 0).reshape(heads * vs, kr)
    index = np.arange(LANES) % rp
    inverse = (10000.0 ** (-(index % (rp // 2)) / (rp // 2))).astype(np.float32)
    sign = np.where(index < rp // 2, -1.0, 1.0).astype(np.float32)
    angle = lengths.astype(f32)[:, None] * inverse[None, :]
    cosine, sine = jnp.cos(angle), jnp.sin(angle) * sign
    w_out_own = w_attn_out.reshape(-1, d_dev)

    first_far = (tokens, gain_in, w_down_q, w_down_kv, w_rope_key.T, w_out_own)
    sums, w_send = call(
        down_kernel,
        [((n_seq, qr + kr + LANES), f32), (w_out_own.shape, f32)],
        scratch=[pltpu.VMEM(a.shape, a.dtype) for a in first_far]
        + [pltpu.SemaphoreType.DMA((len(first_far),))],
        far=first_far,
    )
    crossed = [bit | 1 for bit in higher_bits("kv", 1)]
    w_outs = [w_out_own]
    unsent = list(range(1, lax.axis_size("tp")))

    def send(after, count):
        held, after = lax.optimization_barrier((w_send, after))
        for m in unsent[:count]:
            w_outs.append(swap(held, 0, m))
        del unsent[:count]
        return after

    for mask in [1] + crossed:
        sums = sums + swap(sums, mask)
        if mask == 1:
            sums = send(sums, 1)
        if mask == crossed[0]:
            early = sums
    far = (
        gain_q,
        gain_kv,
        w_nope,
        w_rope,
        w_key,
        w_value,
        latent_cache,
        rope_cache.transpose(0, 2, 1),
        tokens,
        gain_mid,
    )
    gain_q, gain_kv, w_nope, w_rope, w_key, w_value, latent_cache, rope_cache, *kept = call(
        fetch_kernel,
        [(a.shape, a.dtype) for a in far],
        early,
        scratch=[pltpu.SemaphoreType.DMA((len(far),))],
        far=far,
    )
    in_half = heads // 2
    state = (n_seq, in_half * vs + LANES)
    new_latent, new_rope, queries, keep, give = call(
        functools.partial(attend_kernel, heads),
        [
            ((n_seq, kr), bf16),
            ((n_seq, rp), bf16),
            ((kr // LANES + 1, heads * n_seq, LANES), f32),
            (state, f32),
            (state, f32),
        ],
        sums,
        gain_q,
        gain_kv,
        cosine,
        sine,
        angle,
        w_nope,
        w_rope,
        w_key,
        w_value,
        latent_cache,
        rope_cache,
        scratch=[
            pltpu.VMEM((kr // LANES + 1, n_seq * heads, LANES), f32),
            pltpu.VMEM((n_seq, heads, latent_cache.shape[1]), f32),
        ],
    )
    self_scores, self_values = call(
        functools.partial(self_kernel, heads, nope),
        [((2, n_seq, LANES), f32), ((n_seq, heads * vs), f32)],
        new_latent,
        new_rope,
        queries,
        w_value,
    )

    def merge(one, two):
        return call(functools.partial(merge_kernel, in_half), [(state, f32)], one, two)[0]

    part = merge(keep, swap(give, 1))
    for mask in crossed:
        part = send(part, 1 if mask == crossed[0] else len(unsent))
        part = merge(part, swap(part, mask))
    for bit in higher_bits("tp", 0):
        part = merge(part, swap(part, 1, bit))
    other = swap(part, 1)
    half = (n_seq, w_ff_in.shape[1] // 2 + LANES)
    resid_mid, keep, give = call(
        functools.partial(middle_kernel, heads),
        [((n_seq, d_dev), f32), (half, f32), (half, f32)],
        part,
        other,
        self_scores,
        self_values,
        *kept,
        w_ff_in,
        *w_outs,
        scratch=[pltpu.VMEM((lax.axis_size("tp"), n_seq, w_out_own.shape[0]), bf16)],
    )
    sums = keep + swap(give, 1)
    for mask in crossed:
        sums = sums + swap(sums, mask)
    (out,) = call(last_kernel, [((n_seq, d_dev), f32)], sums, swap(sums, 1), w_ff_out)
    for bit in higher_bits("tp", 0):
        out = out + swap(out, 0, bit)
    mixed = (resid_mid + out).astype(bf16)
    return (mixed, new_latent, new_rope)


def solution(mesh):
    return jax.shard_map(
        per_device,
        mesh=mesh,
        in_specs=(
            P(None, "kv"),
            P(),
            P(None, ("kv", "tp"), None),
            P(None, ("kv", "tp"), None),
            P("kv"),
            P("kv", None),
            P("kv", None),
            P("kv", None),
            P(),
            P(),
            P(),
            P(),
            P(),
            P(),
            P("tp", None, "kv"),
            P("kv"),
            P("kv", "tp"),
            P("tp", "kv"),
        ),
        out_specs=(P(None, "kv"), P(), P()),
        check_vma=False,
    )
```

```python
import functools

import jax
import jax.numpy as jnp
import numpy as np
from jax import lax
from jax.experimental import pallas as pl
from jax.experimental.pallas import tpu as pltpu
from jax.sharding import PartitionSpec as P


D = 2048
EPS = 1e-06
LANES = 128
MXU = 256
f32 = jnp.float32
bf16 = jnp.bfloat16
BOTH = ("kv", "tp")


def swap(value, kv_mask, tp_mask=0):
    n_kv, n_tp = lax.axis_size("kv"), lax.axis_size("tp")
    pairs = [
        (k * n_tp + t, (k ^ kv_mask) * n_tp + (t ^ tp_mask)) for k in range(n_kv) for t in range(n_tp)
    ]
    return lax.ppermute(value, BOTH, pairs)


def higher_bits(axis, first):
    size = lax.axis_size(axis)
    assert size & (size - 1) == 0
    return [1 << i for i in range(first, size.bit_length() - 1)]


def paired(terms):
    while len(terms) > 1:
        terms = [one + two for one, two in zip(terms[::2], terms[1::2], strict=True)]
    return terms[0]


def tp_rounds():
    found = higher_bits("tp", 0)
    pairs = [found[i : i + 2] for i in range(0, len(found), 2)]
    return [pair + [sum(pair)] if len(pair) == 2 else pair for pair in pairs]


def parity():
    ones = 0
    for axis in BOTH:
        index = lax.axis_index(axis)
        for i in range(lax.axis_size(axis).bit_length() - 1):
            ones = ones ^ ((index >> i) & 1)
    return ones


def call(kernel, outs, *args, scratch=(), far=()):
    near = pl.BlockSpec(memory_space=pltpu.VMEM)
    return pl.pallas_call(
        kernel,
        out_shape=[pltpu.VMEM(s, t) for s, t in outs],
        in_specs=[near] * len(args) + [pl.BlockSpec(memory_space=pltpu.HBM)] * len(far),
        out_specs=[near] * len(outs),
        scratch_shapes=list(scratch),
        compiler_params=pltpu.CompilerParams(vmem_limit_bytes=16 * 1024 * 1024),
    )(
        *[pltpu.with_memory_space_constraint(a, pltpu.VMEM) for a in args],
        *[pltpu.with_memory_space_constraint(a, pltpu.HBM) for a in far],
    )


def fetched(sources, targets, semaphores):
    copies = [
        pltpu.make_async_copy(source, target, semaphores.at[i])
        for i, (source, target) in enumerate(zip(sources, targets, strict=True))
    ]
    for copy in copies:
        copy.start()
    return copies


def dot(a, b):
    return jnp.dot(a, b, preferred_element_type=f32)


def dot_t(a, b):
    return lax.dot_general(a, b, (((1,), (1,)), ((), ())), preferred_element_type=f32)


def lane(shape):
    return lax.broadcasted_iota(jnp.int32, shape, len(shape) - 1)


def down_kernel(*refs):
    far, (keep, give, send), near, sems = refs[:6], refs[6:9], refs[9:15], refs[15]
    copies = fetched(far, near, sems)
    tokens, gain, w_q, w_kv, w_rope, w_out = near
    copies[0].wait()
    copies[1].wait()
    resid = tokens[...].astype(f32)
    scaled = (resid * gain[...].astype(f32)[None, :]).astype(bf16)
    q, kv = w_q.shape[1], w_kv.shape[1]
    upper = parity() == 1
    half = resid.shape[0] // 2

    def put(begin, end, value):
        keep[:, begin:end] = jnp.where(upper, value[half:], value[:half])
        give[:, begin:end] = jnp.where(upper, value[:half], value[half:])

    copies[2].wait()
    put(0, q, dot(scaled, w_q[...]))
    copies[3].wait()
    put(q, q + kv, dot(scaled, w_kv[...]))
    copies[4].wait()
    tail = dot_t(scaled, w_rope[...])
    square = jnp.sum(resid * resid, axis=1, keepdims=True)
    rest = LANES - tail.shape[1]
    tail = jnp.concatenate([tail, jnp.broadcast_to(square, (tail.shape[0], rest))], axis=1)
    put(q + kv, q + kv + LANES, tail)
    copies[5].wait()
    send[...] = w_out[...].astype(f32)


def fetch_kernel(*refs):
    count = (len(refs) - 2) // 2
    for copy in fetched(refs[1 : 1 + count], refs[1 + count : -1], refs[-1]):
        copy.wait()


def normed(values, gain):
    return values * lax.rsqrt(jnp.mean(values * values, axis=-1, keepdims=True) + EPS) * gain


def gathered(ref, start, count, stride):
    return jnp.concatenate(
        [ref[c, pl.ds(start, count, stride=stride), :] for c in range(ref.shape[0])], axis=1
    )


def rotate(values, cosine, sine, size):
    low = lane(values.shape) % size < size // 2
    other = jnp.where(
        low, pltpu.roll(values, LANES - size // 2, 1), pltpu.roll(values, size // 2, 1)
    )
    return values * cosine + other * sine


def attend_kernel(
    heads,
    own_sums,
    other_sums,
    gain_q,
    gain_kv,
    cosine,
    sine,
    angle,
    w_nope,
    w_rope,
    w_key,
    w_value,
    latent,
    rope,
    new_latent,
    new_rope,
    queries,
    keep,
    give,
    accs,
    scored,
):
    n_seq, rows, kr = latent.shape
    rp = rope.shape[1]
    qr = gain_q.shape[0]
    nope = w_key.shape[0] // heads
    vs = w_value.shape[0] // heads
    scale = (nope + rp) ** (-0.5)
    upper = parity() == 1
    own, other = own_sums[...], other_sums[...]
    sums = jnp.concatenate(
        [jnp.where(upper, other, own), jnp.where(upper, own, other)], axis=0
    )
    tail = sums[:, qr + kr :]
    inv_in = lax.rsqrt(tail[:, LANES - 1 :] / D + EPS)
    query_latent = normed(inv_in * sums[:, :qr], gain_q[...].astype(f32)[None, :]).astype(bf16)
    new_latent[...] = normed(inv_in * sums[:, qr : qr + kr], gain_kv[...].astype(f32)[None, :]).astype(bf16)
    rotated = rotate(inv_in * tail, cosine[...], sine[...], rp)
    new_rope[...] = rotated[:, :rp].astype(bf16)
    up = dot_t(query_latent, w_nope[...])
    per = MXU // nope
    for g in range(heads // per):
        part = up[:, g * MXU : (g + 1) * MXU]
        block = lane(part.shape) // nope
        lhs = jnp.concatenate([jnp.where(block == i, part, 0.0) for i in range(per)], axis=0)
        wide = dot(lhs.astype(bf16), w_key[g * MXU : (g + 1) * MXU, :])
        for c in range(kr // LANES):
            queries[c, g * per * n_seq : (g + 1) * per * n_seq, :] = wide[
                :, c * LANES : (c + 1) * LANES
            ]
    turned = dot_t(query_latent, w_rope[...])
    rotated = jnp.concatenate(
        [
            rotate(turned[:, i : i + LANES], cosine[...], sine[...], rp)
            for i in range(0, heads * rp, LANES)
        ],
        axis=1,
    )
    for h in range(heads):
        queries[kr // LANES, h * n_seq : (h + 1) * n_seq, :rp] = rotated[:, h * rp : (h + 1) * rp]
    first = (lax.axis_index("kv") * lax.axis_size("tp") + lax.axis_index("tp")) * rows
    position = (first + lane((heads, rows))).astype(f32)
    low = lane((heads, LANES)) < LANES // 2
    for s in range(n_seq):
        own = gathered(queries, s, heads, n_seq).astype(bf16)
        scored[s] = (
            dot_t(own[:, :kr], latent[s]) + dot(own[:, kr : kr + rp], rope[s])
        ) * scale
    for s in range(n_seq):
        live = position < angle[s : s + 1, 0:1]
        scores = jnp.where(live, scored[s], -1e30)
        top = jnp.max(scores, axis=1, keepdims=True)
        weights = jnp.where(live, jnp.exp(scores - top), 0.0)
        total = jnp.sum(weights, axis=1, keepdims=True)
        scored[s] = weights
        accs[kr // LANES, s * heads : (s + 1) * heads, :] = jnp.where(low, top, total)
    for s in range(n_seq):
        acc = dot(scored[s].astype(bf16), latent[s])
        for c in range(kr // LANES):
            accs[c, s * heads : (s + 1) * heads, :] = acc[:, c * LANES : (c + 1) * LANES]
    per = MXU // vs
    groups = []
    for g in range(heads // per):
        acc = jnp.concatenate(
            [gathered(accs, g * per + i, n_seq, heads)[:, :kr] for i in range(per)], axis=0
        )
        coarse = acc.astype(bf16)
        fine = (acc - coarse.astype(f32)).astype(bf16)
        wide = dot_t(
            jnp.concatenate([coarse, fine], axis=0), w_value[g * MXU : (g + 1) * MXU, :]
        )
        wide = wide[: per * n_seq] + wide[per * n_seq :]
        block = lane((n_seq, MXU)) // vs
        groups.append(
            sum(
                jnp.where(block == i, wide[i * n_seq : (i + 1) * n_seq, :], 0.0)
                for i in range(per)
            )
        )
    in_half = heads // 2
    place = lane((n_seq, LANES)) % (LANES // 2)
    halves = []
    for half in range(2):
        stats = jnp.zeros((n_seq, LANES), f32)
        for i in range(in_half):
            each = accs[kr // LANES, pl.ds(half * in_half + i, n_seq, stride=heads), :]
            stats = jnp.where(place == i, each, stats)
        mine = groups[half * len(groups) // 2 : (half + 1) * len(groups) // 2]
        halves.append(jnp.concatenate(mine + [stats], axis=1))
    keep[...] = jnp.where(upper, halves[1], halves[0])
    give[...] = jnp.where(upper, halves[0], halves[1])


def spread(factor, heads, width):
    n_seq = factor.shape[0]
    per = LANES // width
    block = lane((n_seq, LANES)) // width
    tiles = []
    for g in range(heads // per):
        tile = jnp.broadcast_to(factor[:, g * per : g * per + 1], (n_seq, LANES))
        for i in range(1, per):
            tile = jnp.where(block == i, factor[:, g * per + i : g * per + i + 1], tile)
        tiles.append(tile)
    return jnp.concatenate(tiles, axis=1)


def merge_kernel(in_half, *refs):
    parts, out = refs[:-1], refs[-1]
    body = out.shape[1] - LANES
    width = body // in_half
    low = lane((out.shape[0], LANES)) < LANES // 2
    stats = [part[:, body:] for part in parts]
    top = functools.reduce(jnp.maximum, stats)
    fades = [jnp.exp(jnp.where(low, each - top, 0.0)) for each in stats]
    total = paired(
        [each * pltpu.roll(fade, LANES // 2, 1) for each, fade in zip(stats, fades, strict=True)]
    )
    out[:, body:] = jnp.where(low, top, total)
    out[:, :body] = paired(
        [
            part[:, :body] * spread(fade, in_half, width)
            for part, fade in zip(parts, fades, strict=True)
        ]
    )


def self_kernel(heads, nope, new_latent, new_rope, queries, w_value, scores, values):
    n_seq, kr = new_latent.shape
    rp = new_rope.shape[1]
    scale = (nope + rp) ** (-0.5)
    key, key_rope = new_latent[...].astype(f32), new_rope[...].astype(f32)
    in_half = heads // 2
    where = lane((n_seq, LANES))
    for half in range(2):
        tile = jnp.zeros((n_seq, LANES), f32)
        for i in range(in_half):
            h = half * in_half + i
            query = jnp.concatenate(
                [queries[c, h * n_seq : (h + 1) * n_seq, :] for c in range(queries.shape[0])],
                axis=1,
            )
            query = query.astype(bf16).astype(f32)
            score = jnp.sum(query[:, :kr] * key, axis=1, keepdims=True) + jnp.sum(
                query[:, kr : kr + rp] * key_rope, axis=1, keepdims=True
            )
            tile = jnp.where(where == i, score * scale, tile)
        scores[half] = tile
    values[...] = dot_t(new_latent[...], w_value[...])


def middle_kernel(
    heads, *refs
):
    (own, other, self_scores, self_values, tokens, gain, w_in), refs = refs[:7], refs[7:]
    n_tp = lax.axis_size("tp")
    w_outs, (mid, keep, give, outs) = refs[:n_tp], refs[n_tp:]
    n_seq = tokens.shape[0]
    in_half = heads // 2
    body = own.shape[1] - LANES
    width = body // in_half
    low = lane((n_seq, LANES)) < LANES // 2
    upper = parity() == 1
    group = w_outs[0].shape[0]
    for half in range(2):
        mine = upper if half == 1 else jnp.logical_not(upper)
        part = jnp.where(mine, own[...], other[...])
        stats = part[:, body:]
        scores = self_scores[half]
        top = jnp.where(low, jnp.maximum(stats, scores), 0.0)
        fade = jnp.exp(jnp.where(low, stats - top, 0.0))
        weight = jnp.exp(jnp.where(low, scores - top, 0.0))
        total = pltpu.roll(stats, LANES // 2, 1) * fade + weight
        total = jnp.where(low, total, 1.0)
        values = self_values[:, half * body : (half + 1) * body]
        joined = part[:, :body] * spread(fade / total, in_half, width) + values * spread(
            weight.astype(bf16).astype(f32) / total, in_half, width
        )
        joined = joined.astype(bf16)
        for g in range(body // group):
            outs[half * (body // group) + g] = joined[:, g * group : (g + 1) * group]
    me = lax.axis_index("tp")
    attn = paired(
        [dot(outs[jnp.bitwise_xor(me, m)], w_outs[m][...].astype(bf16)) for m in range(n_tp)]
    )
    resid_mid = tokens[...].astype(f32) + attn
    mid[...] = resid_mid
    scaled = (resid_mid * gain[...].astype(f32)[None, :]).astype(bf16)
    square = jnp.broadcast_to(jnp.sum(resid_mid * resid_mid, axis=1, keepdims=True), (n_seq, LANES))
    hidden = dot(scaled, w_in[...])
    half = hidden.shape[1] // 2
    keep[:, :half] = jnp.where(upper, hidden[:, half:], hidden[:, :half])
    give[:, :half] = jnp.where(upper, hidden[:, :half], hidden[:, half:])
    keep[:, half:] = square
    give[:, half:] = square


def last_kernel(own, other, w_out, out):
    half = own.shape[1] - LANES
    inv_mid = lax.rsqrt(own[:, half : half + 1] / D + EPS)
    mine = parity()
    total = None
    for part, place in ((own, mine), (other, 1 - mine)):
        hidden = jnp.square(jax.nn.relu(inv_mid * part[:, :half])).astype(bf16)
        begin = pl.multiple_of(place * half, half)
        term = dot(hidden, w_out[pl.ds(begin, half), :])
        total = term if total is None else total + term
    out[...] = total


def per_device(
    tokens,
    lengths,
    latent_cache,
    rope_cache,
    gain_in,
    w_down_q,
    w_down_kv,
    w_rope_key,
    gain_q,
    w_up_qn,
    w_up_qr,
    gain_kv,
    w_key_up,
    w_value_up,
    w_attn_out,
    gain_mid,
    w_ff_in,
    w_ff_out,
):
    n_seq = tokens.shape[0]
    qr, heads, nope = w_up_qn.shape
    rp = w_up_qr.shape[2]
    kr, _, vs = w_value_up.shape
    d_dev = tokens.shape[1]
    w_nope = w_up_qn.transpose(1, 2, 0).reshape(heads * nope, qr)
    w_rope = w_up_qr.transpose(1, 2, 0).reshape(heads * rp, qr)
    w_key = w_key_up.transpose(1, 2, 0).reshape(heads * nope, kr)
    w_value = w_value_up.transpose(1, 2, 0).reshape(heads * vs, kr)
    index = np.arange(LANES) % rp
    inverse = (10000.0 ** (-(index % (rp // 2)) / (rp // 2))).astype(np.float32)
    sign = np.where(index < rp // 2, -1.0, 1.0).astype(np.float32)
    angle = lengths.astype(f32)[:, None] * inverse[None, :]
    cosine, sine = jnp.cos(angle), jnp.sin(angle) * sign
    w_out_own = w_attn_out.reshape(-1, d_dev)

    first_far = (tokens, gain_in, w_down_q, w_down_kv, w_rope_key.T, w_out_own)
    sums_half = (n_seq // 2, qr + kr + LANES)
    keep, give, w_send = call(
        down_kernel,
        [(sums_half, f32), (sums_half, f32), (w_out_own.shape, f32)],
        scratch=[pltpu.VMEM(a.shape, a.dtype) for a in first_far]
        + [pltpu.SemaphoreType.DMA((len(first_far),))],
        far=first_far,
    )
    crossed = [bit | 1 for bit in higher_bits("kv", 1)]
    w_outs = [w_out_own]
    w_outs += [swap(w_send, 0, m) for m in range(1, lax.axis_size("tp"))]
    sums = keep + swap(give, 1)
    early = sums
    for i, mask in enumerate(crossed):
        sums = sums + swap(sums, mask)
        if i == 0:
            early = sums
    far = (
        gain_q,
        gain_kv,
        w_nope,
        w_rope,
        w_key,
        w_value,
        latent_cache,
        rope_cache.transpose(0, 2, 1),
        tokens,
        gain_mid,
    )
    gain_q, gain_kv, w_nope, w_rope, w_key, w_value, latent_cache, rope_cache, *kept = call(
        fetch_kernel,
        [(a.shape, a.dtype) for a in far],
        early,
        scratch=[pltpu.SemaphoreType.DMA((len(far),))],
        far=far,
    )
    gain_kv, sums = lax.optimization_barrier((gain_kv, sums))
    other_sums = swap(sums, 1)
    in_half = heads // 2
    state = (n_seq, in_half * vs + LANES)
    new_latent, new_rope, queries, keep, give = call(
        functools.partial(attend_kernel, heads),
        [
            ((n_seq, kr), bf16),
            ((n_seq, rp), bf16),
            ((kr // LANES + 1, heads * n_seq, LANES), f32),
            (state, f32),
            (state, f32),
        ],
        sums,
        other_sums,
        gain_q,
        gain_kv,
        cosine,
        sine,
        angle,
        w_nope,
        w_rope,
        w_key,
        w_value,
        latent_cache,
        rope_cache,
        scratch=[
            pltpu.VMEM((kr // LANES + 1, n_seq * heads, LANES), f32),
            pltpu.VMEM((n_seq, heads, latent_cache.shape[1]), f32),
        ],
    )
    self_scores, self_values = call(
        functools.partial(self_kernel, heads, nope),
        [((2, n_seq, LANES), f32), ((n_seq, heads * vs), f32)],
        new_latent,
        new_rope,
        queries,
        w_value,
    )

    def merge(*parts):
        return call(functools.partial(merge_kernel, in_half), [(state, f32)], *parts)[0]

    part = merge(keep, swap(give, 1))
    for mask in crossed:
        part = merge(part, swap(part, mask))
    for masks in tp_rounds():
        part = merge(part, *[swap(part, bin(m).count("1") % 2, m) for m in masks])
    other = swap(part, 1)
    half = (n_seq, w_ff_in.shape[1] // 2 + LANES)
    resid_mid, keep, give = call(
        functools.partial(middle_kernel, heads),
        [((n_seq, d_dev), f32), (half, f32), (half, f32)],
        part,
        other,
        self_scores,
        self_values,
        *kept,
        w_ff_in,
        *w_outs,
        scratch=[pltpu.VMEM((lax.axis_size("tp"), n_seq, w_out_own.shape[0]), bf16)],
    )
    sums = keep + swap(give, 1)
    for mask in crossed:
        sums = sums + swap(sums, mask)
    (out,) = call(last_kernel, [((n_seq, d_dev), f32)], sums, swap(sums, 1), w_ff_out)
    for masks in tp_rounds():
        out = paired([out] + [swap(out, 0, m) for m in masks])
    mixed = (resid_mid + out).astype(bf16)
    return (mixed, new_latent, new_rope)


def solution(mesh):
    return sharded(per_device, mesh)


def sharded(step, mesh):
    return jax.shard_map(
        step,
        mesh=mesh,
        in_specs=(
            P(None, "kv"),
            P(),
            P(None, ("kv", "tp"), None),
            P(None, ("kv", "tp"), None),
            P("kv"),
            P("kv", None),
            P("kv", None),
            P("kv", None),
            P(),
            P(),
            P(),
            P(),
            P(),
            P(),
            P("tp", None, "kv"),
            P("kv"),
            P("kv", "tp"),
            P("tp", "kv"),
        ),
        out_specs=(P(None, "kv"), P(), P()),
        check_vma=False,
    )
```

```python
import functools

import jax
import jax.numpy as jnp
import numpy as np
from jax import lax
from jax.experimental import pallas as pl
from jax.experimental.pallas import tpu as pltpu
from jax.sharding import PartitionSpec as P


D = 2048
EPS = 1e-06
LANES = 128
MXU = 256
f32 = jnp.float32
bf16 = jnp.bfloat16
BOTH = ("kv", "tp")


def swap(value, kv_mask, tp_mask=0):
    n_kv, n_tp = lax.axis_size("kv"), lax.axis_size("tp")
    pairs = [
        (k * n_tp + t, (k ^ kv_mask) * n_tp + (t ^ tp_mask)) for k in range(n_kv) for t in range(n_tp)
    ]
    return lax.ppermute(value, BOTH, pairs)


def higher_bits(axis, first):
    size = lax.axis_size(axis)
    assert size & (size - 1) == 0
    return [1 << i for i in range(first, size.bit_length() - 1)]


def paired(terms):
    while len(terms) > 1:
        terms = [one + two for one, two in zip(terms[::2], terms[1::2], strict=True)]
    return terms[0]


def rounds(axis, first):
    found = higher_bits(axis, first)
    pairs = [found[i : i + 2] for i in range(0, len(found), 2)]
    return [pair + [sum(pair)] if len(pair) == 2 else pair for pair in pairs]


def crossing(mask):
    return mask.bit_count() % 2


def parity():
    ones = 0
    for axis in BOTH:
        index = lax.axis_index(axis)
        for i in range(lax.axis_size(axis).bit_length() - 1):
            ones = ones ^ ((index >> i) & 1)
    return ones


def call(kernel, outs, *args, scratch=(), far=()):
    near = pl.BlockSpec(memory_space=pltpu.VMEM)
    return pl.pallas_call(
        kernel,
        out_shape=[pltpu.VMEM(s, t) for s, t in outs],
        in_specs=[near] * len(args) + [pl.BlockSpec(memory_space=pltpu.HBM)] * len(far),
        out_specs=[near] * len(outs),
        scratch_shapes=list(scratch),
        compiler_params=pltpu.CompilerParams(vmem_limit_bytes=16 * 1024 * 1024),
    )(
        *[pltpu.with_memory_space_constraint(a, pltpu.VMEM) for a in args],
        *[pltpu.with_memory_space_constraint(a, pltpu.HBM) for a in far],
    )


def fetched(sources, targets, semaphores):
    copies = [
        pltpu.make_async_copy(source, target, semaphores.at[i])
        for i, (source, target) in enumerate(zip(sources, targets, strict=True))
    ]
    for copy in copies:
        copy.start()
    return copies


def dot(a, b):
    return jnp.dot(a, b, preferred_element_type=f32)


def dot_t(a, b):
    return lax.dot_general(a, b, (((1,), (1,)), ((), ())), preferred_element_type=f32)


def lane(shape):
    return lax.broadcasted_iota(jnp.int32, shape, len(shape) - 1)


def down_kernel(*refs):
    far, (keep, give, send), near, sems = refs[:6], refs[6:9], refs[9:15], refs[15]
    copies = fetched(far, near, sems)
    tokens, gain, w_q, w_kv, w_rope, w_out = near
    copies[0].wait()
    copies[1].wait()
    resid = tokens[...].astype(f32)
    scaled = (resid * gain[...].astype(f32)[None, :]).astype(bf16)
    q, kv = w_q.shape[1], w_kv.shape[1]
    upper = parity() == 1
    half = resid.shape[0] // 2

    def put(begin, end, value):
        keep[:, begin:end] = jnp.where(upper, value[half:], value[:half])
        give[:, begin:end] = jnp.where(upper, value[:half], value[half:])

    copies[2].wait()
    put(0, q, dot(scaled, w_q[...]))
    copies[3].wait()
    put(q, q + kv, dot(scaled, w_kv[...]))
    copies[4].wait()
    tail = dot_t(scaled, w_rope[...])
    square = jnp.sum(resid * resid, axis=1, keepdims=True)
    rest = LANES - tail.shape[1]
    tail = jnp.concatenate([tail, jnp.broadcast_to(square, (tail.shape[0], rest))], axis=1)
    put(q + kv, q + kv + LANES, tail)
    copies[5].wait()
    send[...] = w_out[...].astype(f32)


def fetch_kernel(*refs):
    count = (len(refs) - 2) // 2
    for copy in fetched(refs[1 : 1 + count], refs[1 + count : -1], refs[-1]):
        copy.wait()


def normed(values, gain):
    return values * lax.rsqrt(jnp.mean(values * values, axis=-1, keepdims=True) + EPS) * gain


def gathered(ref, start, count, stride):
    return jnp.concatenate(
        [ref[c, pl.ds(start, count, stride=stride), :] for c in range(ref.shape[0])], axis=1
    )


def rotate(values, cosine, sine, size):
    low = lane(values.shape) % size < size // 2
    other = jnp.where(
        low, pltpu.roll(values, LANES - size // 2, 1), pltpu.roll(values, size // 2, 1)
    )
    return values * cosine + other * sine


def attend_kernel(
    heads,
    own_sums,
    other_sums,
    gain_q,
    gain_kv,
    cosine,
    sine,
    angle,
    w_nope,
    w_rope,
    w_key,
    w_value,
    latent,
    rope,
    new_latent,
    new_rope,
    queries,
    keep,
    give,
    accs,
    scored,
):
    n_seq, rows, kr = latent.shape
    rp = rope.shape[1]
    qr = gain_q.shape[0]
    nope = w_key.shape[0] // heads
    vs = w_value.shape[0] // heads
    scale = (nope + rp) ** (-0.5)
    upper = parity() == 1
    own, other = own_sums[...], other_sums[...]
    sums = jnp.concatenate(
        [jnp.where(upper, other, own), jnp.where(upper, own, other)], axis=0
    )
    tail = sums[:, qr + kr :]
    inv_in = lax.rsqrt(tail[:, LANES - 1 :] / D + EPS)
    query_latent = normed(inv_in * sums[:, :qr], gain_q[...].astype(f32)[None, :]).astype(bf16)
    new_latent[...] = normed(inv_in * sums[:, qr : qr + kr], gain_kv[...].astype(f32)[None, :]).astype(bf16)
    rotated = rotate(inv_in * tail, cosine[...], sine[...], rp)
    new_rope[...] = rotated[:, :rp].astype(bf16)
    up = dot_t(query_latent, w_nope[...])
    per = MXU // nope
    for g in range(heads // per):
        part = up[:, g * MXU : (g + 1) * MXU]
        block = lane(part.shape) // nope
        lhs = jnp.concatenate([jnp.where(block == i, part, 0.0) for i in range(per)], axis=0)
        wide = dot(lhs.astype(bf16), w_key[g * MXU : (g + 1) * MXU, :])
        for c in range(kr // LANES):
            queries[c, g * per * n_seq : (g + 1) * per * n_seq, :] = wide[
                :, c * LANES : (c + 1) * LANES
            ]
    turned = dot_t(query_latent, w_rope[...])
    rotated = jnp.concatenate(
        [
            rotate(turned[:, i : i + LANES], cosine[...], sine[...], rp)
            for i in range(0, heads * rp, LANES)
        ],
        axis=1,
    )
    for h in range(heads):
        queries[kr // LANES, h * n_seq : (h + 1) * n_seq, :rp] = rotated[:, h * rp : (h + 1) * rp]
    first = (lax.axis_index("kv") * lax.axis_size("tp") + lax.axis_index("tp")) * rows
    position = (first + lane((heads, rows))).astype(f32)
    low = lane((heads, LANES)) < LANES // 2
    for s in range(n_seq):
        own = gathered(queries, s, heads, n_seq).astype(bf16)
        scored[s] = (
            dot_t(own[:, :kr], latent[s]) + dot(own[:, kr : kr + rp], rope[s])
        ) * scale
    for s in range(n_seq):
        live = position < angle[s : s + 1, 0:1]
        scores = jnp.where(live, scored[s], -1e30)
        top = jnp.max(scores, axis=1, keepdims=True)
        weights = jnp.where(live, jnp.exp(scores - top), 0.0)
        total = jnp.sum(weights, axis=1, keepdims=True)
        scored[s] = weights
        accs[kr // LANES, s * heads : (s + 1) * heads, :] = jnp.where(low, top, total)
    for s in range(n_seq):
        acc = dot(scored[s].astype(bf16), latent[s])
        for c in range(kr // LANES):
            accs[c, s * heads : (s + 1) * heads, :] = acc[:, c * LANES : (c + 1) * LANES]
    per = MXU // vs
    groups = []
    for g in range(heads // per):
        acc = jnp.concatenate(
            [gathered(accs, g * per + i, n_seq, heads)[:, :kr] for i in range(per)], axis=0
        )
        coarse = acc.astype(bf16)
        fine = (acc - coarse.astype(f32)).astype(bf16)
        wide = dot_t(
            jnp.concatenate([coarse, fine], axis=0), w_value[g * MXU : (g + 1) * MXU, :]
        )
        wide = wide[: per * n_seq] + wide[per * n_seq :]
        block = lane((n_seq, MXU)) // vs
        groups.append(
            sum(
                jnp.where(block == i, wide[i * n_seq : (i + 1) * n_seq, :], 0.0)
                for i in range(per)
            )
        )
    in_half = heads // 2
    place = lane((n_seq, LANES)) % (LANES // 2)
    halves = []
    for half in range(2):
        stats = jnp.zeros((n_seq, LANES), f32)
        for i in range(in_half):
            each = accs[kr // LANES, pl.ds(half * in_half + i, n_seq, stride=heads), :]
            stats = jnp.where(place == i, each, stats)
        mine = groups[half * len(groups) // 2 : (half + 1) * len(groups) // 2]
        halves.append(jnp.concatenate(mine + [stats], axis=1))
    keep[...] = jnp.where(upper, halves[1], halves[0])
    give[...] = jnp.where(upper, halves[0], halves[1])


def spread(factor, heads, width):
    n_seq = factor.shape[0]
    per = LANES // width
    block = lane((n_seq, LANES)) // width
    tiles = []
    for g in range(heads // per):
        tile = jnp.broadcast_to(factor[:, g * per : g * per + 1], (n_seq, LANES))
        for i in range(1, per):
            tile = jnp.where(block == i, factor[:, g * per + i : g * per + i + 1], tile)
        tiles.append(tile)
    return jnp.concatenate(tiles, axis=1)


def merge_kernel(in_half, *refs):
    parts, out = refs[:-1], refs[-1]
    body = out.shape[1] - LANES
    width = body // in_half
    low = lane((out.shape[0], LANES)) < LANES // 2
    stats = [part[:, body:] for part in parts]
    top = functools.reduce(jnp.maximum, stats)
    fades = [jnp.exp(jnp.where(low, each - top, 0.0)) for each in stats]
    total = paired(
        [each * pltpu.roll(fade, LANES // 2, 1) for each, fade in zip(stats, fades, strict=True)]
    )
    out[:, body:] = jnp.where(low, top, total)
    out[:, :body] = paired(
        [
            part[:, :body] * spread(fade, in_half, width)
            for part, fade in zip(parts, fades, strict=True)
        ]
    )


def self_kernel(heads, nope, new_latent, new_rope, queries, w_value, scores, values):
    n_seq, kr = new_latent.shape
    rp = new_rope.shape[1]
    scale = (nope + rp) ** (-0.5)
    key, key_rope = new_latent[...].astype(f32), new_rope[...].astype(f32)
    in_half = heads // 2
    where = lane((n_seq, LANES))
    for half in range(2):
        tile = jnp.zeros((n_seq, LANES), f32)
        for i in range(in_half):
            h = half * in_half + i
            query = jnp.concatenate(
                [queries[c, h * n_seq : (h + 1) * n_seq, :] for c in range(queries.shape[0])],
                axis=1,
            )
            query = query.astype(bf16).astype(f32)
            score = jnp.sum(query[:, :kr] * key, axis=1, keepdims=True) + jnp.sum(
                query[:, kr : kr + rp] * key_rope, axis=1, keepdims=True
            )
            tile = jnp.where(where == i, score * scale, tile)
        scores[half] = tile
    values[...] = dot_t(new_latent[...], w_value[...])


def middle_kernel(
    heads, *refs
):
    (own, other, self_scores, self_values, tokens, gain, w_in), refs = refs[:7], refs[7:]
    n_tp = lax.axis_size("tp")
    w_outs, (mid, keep, give, outs) = refs[:n_tp], refs[n_tp:]
    n_seq = tokens.shape[0]
    in_half = heads // 2
    body = own.shape[1] - LANES
    width = body // in_half
    low = lane((n_seq, LANES)) < LANES // 2
    upper = parity() == 1
    group = w_outs[0].shape[0]
    for half in range(2):
        mine = upper if half == 1 else jnp.logical_not(upper)
        part = jnp.where(mine, own[...], other[...])
        stats = part[:, body:]
        scores = self_scores[half]
        top = jnp.where(low, jnp.maximum(stats, scores), 0.0)
        fade = jnp.exp(jnp.where(low, stats - top, 0.0))
        weight = jnp.exp(jnp.where(low, scores - top, 0.0))
        total = pltpu.roll(stats, LANES // 2, 1) * fade + weight
        total = jnp.where(low, total, 1.0)
        values = self_values[:, half * body : (half + 1) * body]
        joined = part[:, :body] * spread(fade / total, in_half, width) + values * spread(
            weight.astype(bf16).astype(f32) / total, in_half, width
        )
        joined = joined.astype(bf16)
        for g in range(body // group):
            outs[half * (body // group) + g] = joined[:, g * group : (g + 1) * group]
    me = lax.axis_index("tp")
    attn = paired(
        [dot(outs[jnp.bitwise_xor(me, m)], w_outs[m][...].astype(bf16)) for m in range(n_tp)]
    )
    resid_mid = tokens[...].astype(f32) + attn
    mid[...] = resid_mid
    scaled = (resid_mid * gain[...].astype(f32)[None, :]).astype(bf16)
    square = jnp.sum(resid_mid * resid_mid, axis=1, keepdims=True)
    hidden = dot(scaled, w_in[...])
    half = hidden.shape[1] // 2
    for i in range(half // LANES):
        one = hidden[:, i * LANES : (i + 1) * LANES]
        two = hidden[:, half + i * LANES : half + (i + 1) * LANES]
        keep[i * n_seq : (i + 1) * n_seq, :] = jnp.where(upper, two, one)
        give[i * n_seq : (i + 1) * n_seq, :] = jnp.where(upper, one, two)
    few = n_seq // 2
    squares = jnp.where(lane((few, LANES)) < LANES // 2, square[:few], square[few:])
    keep[half // LANES * n_seq :, :] = squares
    give[half // LANES * n_seq :, :] = squares


def last_kernel(own, other, w_out, out):
    n_seq = out.shape[0]
    tiles = own.shape[0] // n_seq
    half = tiles * LANES
    squares = own[tiles * n_seq :, :]
    square = jnp.concatenate([squares[:, :1], squares[:, LANES // 2 : LANES // 2 + 1]], axis=0)
    inv_mid = lax.rsqrt(square / D + EPS)
    mine = parity()
    total = None
    for part, place in ((own, mine), (other, 1 - mine)):
        hidden = jnp.concatenate(
            [part[i * n_seq : (i + 1) * n_seq, :] for i in range(tiles)], axis=1
        )
        hidden = jnp.square(jax.nn.relu(inv_mid * hidden)).astype(bf16)
        begin = pl.multiple_of(place * half, half)
        term = dot(hidden, w_out[pl.ds(begin, half), :])
        total = term if total is None else total + term
    out[...] = total


def per_device(
    tokens,
    lengths,
    latent_cache,
    rope_cache,
    gain_in,
    w_down_q,
    w_down_kv,
    w_rope_key,
    gain_q,
    w_up_qn,
    w_up_qr,
    gain_kv,
    w_key_up,
    w_value_up,
    w_attn_out,
    gain_mid,
    w_ff_in,
    w_ff_out,
):
    n_seq = tokens.shape[0]
    qr, heads, nope = w_up_qn.shape
    rp = w_up_qr.shape[2]
    kr, _, vs = w_value_up.shape
    d_dev = tokens.shape[1]
    w_nope = w_up_qn.transpose(1, 2, 0).reshape(heads * nope, qr)
    w_rope = w_up_qr.transpose(1, 2, 0).reshape(heads * rp, qr)
    w_key = w_key_up.transpose(1, 2, 0).reshape(heads * nope, kr)
    w_value = w_value_up.transpose(1, 2, 0).reshape(heads * vs, kr)
    index = np.arange(LANES) % rp
    inverse = (10000.0 ** (-(index % (rp // 2)) / (rp // 2))).astype(np.float32)
    sign = np.where(index < rp // 2, -1.0, 1.0).astype(np.float32)
    angle = lengths.astype(f32)[:, None] * inverse[None, :]
    cosine, sine = jnp.cos(angle), jnp.sin(angle) * sign
    w_out_own = w_attn_out.reshape(-1, d_dev)

    first_far = (tokens, gain_in, w_down_q, w_down_kv, w_rope_key.T, w_out_own)
    sums_half = (n_seq // 2, qr + kr + LANES)
    keep, give, w_send = call(
        down_kernel,
        [(sums_half, f32), (sums_half, f32), (w_out_own.shape, f32)],
        scratch=[pltpu.VMEM(a.shape, a.dtype) for a in first_far]
        + [pltpu.SemaphoreType.DMA((len(first_far),))],
        far=first_far,
    )
    kv_rounds, tp_rounds = rounds("kv", 1), rounds("tp", 0)
    w_outs = [w_out_own]
    w_outs += [swap(w_send, 0, m) for m in range(1, lax.axis_size("tp"))]
    sums = keep + swap(give, 1)
    early = sums
    for bit in higher_bits("kv", 1):
        sums = sums + swap(sums, bit | 1)
        if bit == 2:
            early = sums
    far = (
        gain_q,
        gain_kv,
        w_nope,
        w_rope,
        w_key,
        w_value,
        latent_cache,
        rope_cache.transpose(0, 2, 1),
        tokens,
        gain_mid,
    )
    gain_q, gain_kv, w_nope, w_rope, w_key, w_value, latent_cache, rope_cache, *kept = call(
        fetch_kernel,
        [(a.shape, a.dtype) for a in far],
        early,
        scratch=[pltpu.SemaphoreType.DMA((len(far),))],
        far=far,
    )
    gain_kv, sums = lax.optimization_barrier((gain_kv, sums))
    other_sums = swap(sums, 1)
    in_half = heads // 2
    state = (n_seq, in_half * vs + LANES)
    new_latent, new_rope, queries, keep, give = call(
        functools.partial(attend_kernel, heads),
        [
            ((n_seq, kr), bf16),
            ((n_seq, rp), bf16),
            ((kr // LANES + 1, heads * n_seq, LANES), f32),
            (state, f32),
            (state, f32),
        ],
        sums,
        other_sums,
        gain_q,
        gain_kv,
        cosine,
        sine,
        angle,
        w_nope,
        w_rope,
        w_key,
        w_value,
        latent_cache,
        rope_cache,
        scratch=[
            pltpu.VMEM((kr // LANES + 1, n_seq * heads, LANES), f32),
            pltpu.VMEM((n_seq, heads, latent_cache.shape[1]), f32),
        ],
    )
    self_scores, self_values = call(
        functools.partial(self_kernel, heads, nope),
        [((2, n_seq, LANES), f32), ((n_seq, heads * vs), f32)],
        new_latent,
        new_rope,
        queries,
        w_value,
    )

    def merge(*parts):
        return call(functools.partial(merge_kernel, in_half), [(state, f32)], *parts)[0]

    part = merge(keep, swap(give, 1))
    for masks in kv_rounds:
        part = merge(part, *[swap(part, m | crossing(m)) for m in masks])
    for masks in tp_rounds:
        part = merge(part, *[swap(part, crossing(m), m) for m in masks])
    other = swap(part, 1)
    half = (w_ff_in.shape[1] // 2 // LANES * n_seq + n_seq // 2, LANES)
    resid_mid, keep, give = call(
        functools.partial(middle_kernel, heads),
        [((n_seq, d_dev), f32), (half, f32), (half, f32)],
        part,
        other,
        self_scores,
        self_values,
        *kept,
        w_ff_in,
        *w_outs,
        scratch=[pltpu.VMEM((lax.axis_size("tp"), n_seq, w_out_own.shape[0]), bf16)],
    )
    sums = keep + swap(give, 1)
    for masks in kv_rounds:
        sums = paired([sums] + [swap(sums, m | crossing(m)) for m in masks])
    (out,) = call(last_kernel, [((n_seq, d_dev), f32)], sums, swap(sums, 1), w_ff_out)
    for masks in tp_rounds:
        out = paired([out] + [swap(out, 0, m) for m in masks])
    mixed = (resid_mid + out).astype(bf16)
    return (mixed, new_latent, new_rope)


def solution(mesh):
    return sharded(per_device, mesh)


def sharded(step, mesh):
    return jax.shard_map(
        step,
        mesh=mesh,
        in_specs=(
            P(None, "kv"),
            P(),
            P(None, ("kv", "tp"), None),
            P(None, ("kv", "tp"), None),
            P("kv"),
            P("kv", None),
            P("kv", None),
            P("kv", None),
            P(),
            P(),
            P(),
            P(),
            P(),
            P(),
            P("tp", None, "kv"),
            P("kv"),
            P("kv", "tp"),
            P("tp", "kv"),
        ),
        out_specs=(P(None, "kv"), P(), P()),
        check_vma=False,
    )
```

```python
import functools

import jax
import jax.numpy as jnp
import numpy as np
from jax import lax
from jax.experimental import pallas as pl
from jax.experimental.pallas import tpu as pltpu
from jax.sharding import PartitionSpec as P


D = 2048
EPS = 1e-06
LANES = 128
MXU = 256
f32 = jnp.float32
bf16 = jnp.bfloat16
BOTH = ("kv", "tp")


def swap(value, kv_mask, tp_mask=0):
    n_kv, n_tp = lax.axis_size("kv"), lax.axis_size("tp")
    pairs = [
        (k * n_tp + t, (k ^ kv_mask) * n_tp + (t ^ tp_mask)) for k in range(n_kv) for t in range(n_tp)
    ]
    return lax.ppermute(value, BOTH, pairs)


def higher_bits(axis, first):
    size = lax.axis_size(axis)
    assert size & (size - 1) == 0
    return [1 << i for i in range(first, size.bit_length() - 1)]


def paired(terms):
    while len(terms) > 1:
        terms = [one + two for one, two in zip(terms[::2], terms[1::2], strict=True)]
    return terms[0]


def rounds(axis, first):
    found = higher_bits(axis, first)
    pairs = [found[i : i + 2] for i in range(0, len(found), 2)]
    return [pair + [sum(pair)] if len(pair) == 2 else pair for pair in pairs]


def crossing(mask):
    return mask.bit_count() % 2


def parity():
    ones = 0
    for axis in BOTH:
        index = lax.axis_index(axis)
        for i in range(lax.axis_size(axis).bit_length() - 1):
            ones = ones ^ ((index >> i) & 1)
    return ones


def call(kernel, outs, *args, scratch=(), far=()):
    near = pl.BlockSpec(memory_space=pltpu.VMEM)
    return pl.pallas_call(
        kernel,
        out_shape=[pltpu.VMEM(s, t) for s, t in outs],
        in_specs=[near] * len(args) + [pl.BlockSpec(memory_space=pltpu.HBM)] * len(far),
        out_specs=[near] * len(outs),
        scratch_shapes=list(scratch),
        compiler_params=pltpu.CompilerParams(vmem_limit_bytes=16 * 1024 * 1024),
    )(
        *[pltpu.with_memory_space_constraint(a, pltpu.VMEM) for a in args],
        *[pltpu.with_memory_space_constraint(a, pltpu.HBM) for a in far],
    )


def fetched(sources, targets, semaphores):
    copies = [
        pltpu.make_async_copy(source, target, semaphores.at[i])
        for i, (source, target) in enumerate(zip(sources, targets, strict=True))
    ]
    for copy in copies:
        copy.start()
    return copies


def dot(a, b):
    return jnp.dot(a, b, preferred_element_type=f32)


def dot_t(a, b):
    return lax.dot_general(a, b, (((1,), (1,)), ((), ())), preferred_element_type=f32)


def lane(shape):
    return lax.broadcasted_iota(jnp.int32, shape, len(shape) - 1)


def down_kernel(*refs):
    far, (keep, give, send, keys), near, sems = refs[:8], refs[8:12], refs[12:20], refs[20]
    tokens, gain, w_q, w_kv, w_rope, w_out, latent, rope = near
    few, rows, _ = latent.shape
    theirs = pl.ds((1 - parity()) * few, few)
    copies = fetched([*far[:6], far[6].at[theirs], far[7].at[theirs]], near, sems)
    copies[0].wait()
    copies[1].wait()
    resid = tokens[...].astype(f32)
    scaled = (resid * gain[...].astype(f32)[None, :]).astype(bf16)
    q, kv = w_q.shape[1], w_kv.shape[1]
    upper = parity() == 1
    half = resid.shape[0] // 2

    def put(begin, end, value):
        keep[:, begin:end] = jnp.where(upper, value[half:], value[:half])
        give[:, begin:end] = jnp.where(upper, value[:half], value[half:])

    copies[2].wait()
    put(0, q, dot(scaled, w_q[...]))
    copies[3].wait()
    put(q, q + kv, dot(scaled, w_kv[...]))
    copies[4].wait()
    tail = dot_t(scaled, w_rope[...])
    square = jnp.sum(resid * resid, axis=1, keepdims=True)
    rest = LANES - tail.shape[1]
    tail = jnp.concatenate([tail, jnp.broadcast_to(square, (tail.shape[0], rest))], axis=1)
    put(q + kv, q + kv + LANES, tail)
    copies[5].wait()
    send[...] = w_out[...].astype(f32)
    copies[6].wait()
    keys[:, :rows, :] = latent[...].astype(f32)
    copies[7].wait()
    spare = jnp.zeros((rope.shape[1], latent.shape[2] - rows), f32)
    for s in range(few):
        keys[s, rows:, :] = jnp.concatenate([rope[s].astype(f32), spare], axis=1)


def fetch_kernel(halved, *refs):
    count = (len(refs) - 2) // 2
    sources, targets = list(refs[1 : 1 + count]), refs[1 + count : -1]
    for i in range(count - halved, count):
        few = targets[i].shape[0]
        sources[i] = sources[i].at[pl.ds(parity() * few, few)]
    for copy in fetched(sources, targets, refs[-1]):
        copy.wait()


def normed(values, gain):
    return values * lax.rsqrt(jnp.mean(values * values, axis=-1, keepdims=True) + EPS) * gain


def gathered(ref, start, count, stride):
    return jnp.concatenate(
        [ref[c, pl.ds(start, count, stride=stride), :] for c in range(ref.shape[0])], axis=1
    )


def rotate(values, cosine, sine, size):
    low = lane(values.shape) % size < size // 2
    other = jnp.where(
        low, pltpu.roll(values, LANES - size // 2, 1), pltpu.roll(values, size // 2, 1)
    )
    return values * cosine + other * sine


def fresh(sums, gain, cosine, sine, qr, kr, rp):
    tail = sums[:, qr + kr :]
    inv_in = lax.rsqrt(tail[:, LANES - 1 :] / D + EPS)
    latent = normed(inv_in * sums[:, qr : qr + kr], gain.astype(f32)[None, :]).astype(bf16)
    return latent, rotate(inv_in * tail, cosine, sine, rp)[:, :rp].astype(bf16)


def fresh_kernel(qr, own_sums, other_sums, gain_kv, cosine, sine, new_latent, new_rope):
    upper = parity() == 1
    own, other = own_sums[...], other_sums[...]
    sums = jnp.concatenate([jnp.where(upper, other, own), jnp.where(upper, own, other)], axis=0)
    new_latent[...], new_rope[...] = fresh(
        sums, gain_kv[...], cosine[...], sine[...], qr, new_latent.shape[1], new_rope.shape[1]
    )


def attend_kernel(
    heads,
    own_sums,
    gain_q,
    gain_kv,
    cosines,
    sines,
    angles,
    w_nope,
    w_rope,
    w_key,
    w_value,
    latent,
    rope,
    keys,
    new_latent,
    new_rope,
    queries,
    partial,
    accs,
    scored,
    theirs,
):
    n_seq, rows, kr = latent.shape
    rp = rope.shape[1]
    qr = gain_q.shape[0]
    nope = w_key.shape[0] // heads
    vs = w_value.shape[0] // heads
    scale = (nope + rp) ** (-0.5)
    mine = pl.ds(pl.multiple_of(parity() * n_seq, n_seq), n_seq)
    cosine, sine, angle = cosines[mine, :], sines[mine, :], angles[mine, :]
    sums = own_sums[...]
    theirs[...] = keys[:, :rows, :].astype(bf16)
    new_latent[...], new_rope[...] = fresh(sums, gain_kv[...], cosine, sine, qr, kr, rp)
    inv_in = lax.rsqrt(sums[:, qr + kr + LANES - 1 :] / D + EPS)
    query_latent = normed(inv_in * sums[:, :qr], gain_q[...].astype(f32)[None, :]).astype(bf16)
    up = dot_t(query_latent, w_nope[...])
    per = MXU // nope
    for g in range(heads // per):
        part = up[:, g * MXU : (g + 1) * MXU]
        block = lane(part.shape) // nope
        lhs = jnp.concatenate([jnp.where(block == i, part, 0.0) for i in range(per)], axis=0)
        wide = dot(lhs.astype(bf16), w_key[g * MXU : (g + 1) * MXU, :])
        for c in range(kr // LANES):
            queries[c, g * per * n_seq : (g + 1) * per * n_seq, :] = wide[
                :, c * LANES : (c + 1) * LANES
            ]
    turned = dot_t(query_latent, w_rope[...])
    rotated = jnp.concatenate(
        [
            rotate(turned[:, i : i + LANES], cosine, sine, rp)
            for i in range(0, heads * rp, LANES)
        ],
        axis=1,
    )
    for h in range(heads):
        queries[kr // LANES, h * n_seq : (h + 1) * n_seq, :rp] = rotated[:, h * rp : (h + 1) * rp]
    core, column, width = lax.axis_index("kv"), lax.axis_index("tp"), lax.axis_size("tp")
    places = [
        (index * width + column) * rows + lane((heads, rows))
        for index in (core, jnp.bitwise_xor(core, 1))
    ]
    low = lane((heads, LANES)) < LANES // 2
    for s in range(n_seq):
        own = gathered(queries, s, heads, n_seq).astype(bf16)
        nopes, ropes = own[:, :kr], own[:, kr : kr + rp]
        scored[0, s] = (dot_t(nopes, latent[s]) + dot(ropes, rope[s])) * scale
        turned_keys = keys[s, rows:, :rows].astype(bf16)
        scored[1, s] = (dot_t(nopes, theirs[s]) + dot(ropes, turned_keys)) * scale
    for s in range(n_seq):
        live = [place.astype(f32) < angle[s : s + 1, 0:1] for place in places]
        scores = [jnp.where(live[i], scored[i, s], -1e30) for i in range(2)]
        top = jnp.max(jnp.maximum(*scores), axis=1, keepdims=True)
        weights = [jnp.where(live[i], jnp.exp(scores[i] - top), 0.0) for i in range(2)]
        total = jnp.sum(weights[0] + weights[1], axis=1, keepdims=True)
        for i in range(2):
            scored[i, s] = weights[i]
        accs[kr // LANES, s * heads : (s + 1) * heads, :] = jnp.where(low, top, total)
    for s in range(n_seq):
        acc = dot(scored[0, s].astype(bf16), latent[s]) + dot(scored[1, s].astype(bf16), theirs[s])
        for c in range(kr // LANES):
            accs[c, s * heads : (s + 1) * heads, :] = acc[:, c * LANES : (c + 1) * LANES]
    per = MXU // vs
    groups = []
    for g in range(heads // per):
        acc = jnp.concatenate(
            [gathered(accs, g * per + i, n_seq, heads)[:, :kr] for i in range(per)], axis=0
        )
        coarse = acc.astype(bf16)
        fine = (acc - coarse.astype(f32)).astype(bf16)
        wide = dot_t(
            jnp.concatenate([coarse, fine], axis=0), w_value[g * MXU : (g + 1) * MXU, :]
        )
        wide = wide[: per * n_seq] + wide[per * n_seq :]
        block = lane((n_seq, MXU)) // vs
        groups.append(
            sum(
                jnp.where(block == i, wide[i * n_seq : (i + 1) * n_seq, :], 0.0)
                for i in range(per)
            )
        )
    place = lane((n_seq, LANES)) % (LANES // 2)
    stats = jnp.zeros((n_seq, LANES), f32)
    for h in range(heads):
        each = accs[kr // LANES, pl.ds(h, n_seq, stride=heads), :]
        stats = jnp.where(place == h, each, stats)
    partial[...] = jnp.concatenate(groups + [stats], axis=1)


def spread(factor, heads, width):
    n_seq = factor.shape[0]
    per = LANES // width
    block = lane((n_seq, LANES)) // width
    tiles = []
    for g in range(heads // per):
        tile = jnp.broadcast_to(factor[:, g * per : g * per + 1], (n_seq, LANES))
        for i in range(1, per):
            tile = jnp.where(block == i, factor[:, g * per + i : g * per + i + 1], tile)
        tiles.append(tile)
    return jnp.concatenate(tiles, axis=1)


def merge_kernel(heads, *refs):
    parts, out = refs[:-1], refs[-1]
    body = out.shape[1] - LANES
    width = body // heads
    low = lane((out.shape[0], LANES)) < LANES // 2
    stats = [part[:, body:] for part in parts]
    top = functools.reduce(jnp.maximum, stats)
    fades = [jnp.exp(jnp.where(low, each - top, 0.0)) for each in stats]
    total = paired(
        [each * pltpu.roll(fade, LANES // 2, 1) for each, fade in zip(stats, fades, strict=True)]
    )
    out[:, body:] = jnp.where(low, top, total)
    out[:, :body] = paired(
        [
            part[:, :body] * spread(fade, heads, width)
            for part, fade in zip(parts, fades, strict=True)
        ]
    )


def self_kernel(heads, nope, new_latent, new_rope, queries, w_value, scores, values):
    n_seq, kr = new_latent.shape
    rp = new_rope.shape[1]
    scale = (nope + rp) ** (-0.5)
    key, key_rope = new_latent[...].astype(f32), new_rope[...].astype(f32)
    where = lane((n_seq, LANES))
    tile = jnp.zeros((n_seq, LANES), f32)
    for h in range(heads):
        query = jnp.concatenate(
            [queries[c, h * n_seq : (h + 1) * n_seq, :] for c in range(queries.shape[0])], axis=1
        )
        query = query.astype(bf16).astype(f32)
        score = jnp.sum(query[:, :kr] * key, axis=1, keepdims=True) + jnp.sum(
            query[:, kr : kr + rp] * key_rope, axis=1, keepdims=True
        )
        tile = jnp.where(where == h, score * scale, tile)
    scores[...] = tile
    values[...] = dot_t(new_latent[...], w_value[...])


def finish_kernel(heads, part, self_scores, self_values, out):
    body = out.shape[1]
    width = body // heads
    low = lane(self_scores.shape) < LANES // 2
    stats, scores = part[:, body:], self_scores[...]
    top = jnp.where(low, jnp.maximum(stats, scores), 0.0)
    fade = jnp.exp(jnp.where(low, stats - top, 0.0))
    weight = jnp.exp(jnp.where(low, scores - top, 0.0))
    total = pltpu.roll(stats, LANES // 2, 1) * fade + weight
    total = jnp.where(lane(total.shape) < heads, total, 1.0)
    joined = part[:, :body] * spread(fade / total, heads, width) + self_values[...] * spread(
        weight.astype(bf16).astype(f32) / total, heads, width
    )
    out[...] = joined.astype(bf16).astype(f32)


def middle_kernel(*refs):
    (own, other, tokens, gain, w_in), refs = refs[:5], refs[5:]
    n_tp = lax.axis_size("tp")
    w_outs, (mid, keep, give, outs) = refs[:n_tp], refs[n_tp:]
    n_seq = tokens.shape[0]
    upper = parity() == 1
    group = w_outs[0].shape[0]
    joined = jnp.concatenate(
        [jnp.where(upper, other[...], own[...]), jnp.where(upper, own[...], other[...])], axis=0
    ).astype(bf16)
    for g in range(joined.shape[1] // group):
        outs[g] = joined[:, g * group : (g + 1) * group]
    me = lax.axis_index("tp")
    attn = paired(
        [dot(outs[jnp.bitwise_xor(me, m)], w_outs[m][...].astype(bf16)) for m in range(n_tp)]
    )
    resid_mid = tokens[...].astype(f32) + attn
    mid[...] = resid_mid
    scaled = (resid_mid * gain[...].astype(f32)[None, :]).astype(bf16)
    square = jnp.sum(resid_mid * resid_mid, axis=1, keepdims=True)
    hidden = dot(scaled, w_in[...])
    half = hidden.shape[1] // 2
    for i in range(half // LANES):
        one = hidden[:, i * LANES : (i + 1) * LANES]
        two = hidden[:, half + i * LANES : half + (i + 1) * LANES]
        keep[i * n_seq : (i + 1) * n_seq, :] = jnp.where(upper, two, one)
        give[i * n_seq : (i + 1) * n_seq, :] = jnp.where(upper, one, two)
    few = n_seq // 2
    squares = jnp.where(lane((few, LANES)) < LANES // 2, square[:few], square[few:])
    keep[half // LANES * n_seq :, :] = squares
    give[half // LANES * n_seq :, :] = squares


def last_kernel(own, other, w_out, out):
    n_seq = out.shape[0]
    tiles = own.shape[0] // n_seq
    half = tiles * LANES
    squares = own[tiles * n_seq :, :]
    square = jnp.concatenate([squares[:, :1], squares[:, LANES // 2 : LANES // 2 + 1]], axis=0)
    inv_mid = lax.rsqrt(square / D + EPS)
    mine = parity()
    total = None
    for part, place in ((own, mine), (other, 1 - mine)):
        hidden = jnp.concatenate(
            [part[i * n_seq : (i + 1) * n_seq, :] for i in range(tiles)], axis=1
        )
        hidden = jnp.square(jax.nn.relu(inv_mid * hidden)).astype(bf16)
        begin = pl.multiple_of(place * half, half)
        term = dot(hidden, w_out[pl.ds(begin, half), :])
        total = term if total is None else total + term
    out[...] = total


def per_device(
    tokens,
    lengths,
    latent_cache,
    rope_cache,
    gain_in,
    w_down_q,
    w_down_kv,
    w_rope_key,
    gain_q,
    w_up_qn,
    w_up_qr,
    gain_kv,
    w_key_up,
    w_value_up,
    w_attn_out,
    gain_mid,
    w_ff_in,
    w_ff_out,
):
    n_seq = tokens.shape[0]
    qr, heads, nope = w_up_qn.shape
    rp = w_up_qr.shape[2]
    kr, _, vs = w_value_up.shape
    d_dev = tokens.shape[1]
    w_nope = w_up_qn.transpose(1, 2, 0).reshape(heads * nope, qr)
    w_rope = w_up_qr.transpose(1, 2, 0).reshape(heads * rp, qr)
    w_key = w_key_up.transpose(1, 2, 0).reshape(heads * nope, kr)
    w_value = w_value_up.transpose(1, 2, 0).reshape(heads * vs, kr)
    index = np.arange(LANES) % rp
    inverse = (10000.0 ** (-(index % (rp // 2)) / (rp // 2))).astype(np.float32)
    sign = np.where(index < rp // 2, -1.0, 1.0).astype(np.float32)
    angle = lengths.astype(f32)[:, None] * inverse[None, :]
    cosine, sine = jnp.cos(angle), jnp.sin(angle) * sign
    w_out_own = w_attn_out.reshape(-1, d_dev)

    ropes = rope_cache.transpose(0, 2, 1)
    few = n_seq // 2
    latent_half = (few, *latent_cache.shape[1:])
    rope_half = (few, *ropes.shape[1:])
    first_far = (tokens, gain_in, w_down_q, w_down_kv, w_rope_key.T, w_out_own, latent_cache, ropes)
    first_near = [(a.shape, a.dtype) for a in first_far[:6]]
    first_near += [(latent_half, bf16), (rope_half, bf16)]
    keys_shape = (few, latent_half[1] + rope_half[1], kr)
    sums_half = (n_seq // 2, qr + kr + LANES)
    keep, give, w_send, keys = call(
        down_kernel,
        [(sums_half, f32), (sums_half, f32), (w_out_own.shape, f32), (keys_shape, f32)],
        scratch=[pltpu.VMEM(*a) for a in first_near]
        + [pltpu.SemaphoreType.DMA((len(first_far),))],
        far=first_far,
    )
    kv_rounds, tp_rounds = rounds("kv", 1), rounds("tp", 0)
    w_outs = [w_out_own]
    w_outs += [swap(w_send, 0, m) for m in range(1, lax.axis_size("tp"))]
    sums = keep + swap(give, 1)
    keys = swap(keys, 1)
    early = sums
    for bit in higher_bits("kv", 1):
        sums = sums + swap(sums, bit | 1)
        if bit == 2:
            early = sums
    far = (
        gain_q,
        gain_kv,
        w_nope,
        w_rope,
        w_key,
        w_value,
        tokens,
        gain_mid,
        latent_cache,
        ropes,
    )
    shapes = [(a.shape, a.dtype) for a in far[:-2]] + [(latent_half, bf16), (rope_half, bf16)]
    gain_q, gain_kv, w_nope, w_rope, w_key, w_value, *kept, latents, ropes = call(
        functools.partial(fetch_kernel, 2),
        shapes,
        early,
        scratch=[pltpu.SemaphoreType.DMA((len(far),))],
        far=far,
    )
    other_sums = swap(sums, 1)
    state = (few, heads * vs + LANES)
    latent_new, rope_new, queries, part = call(
        functools.partial(attend_kernel, heads),
        [
            ((few, kr), bf16),
            ((few, rp), bf16),
            ((kr // LANES + 1, heads * few, LANES), f32),
            (state, f32),
        ],
        sums,
        gain_q,
        gain_kv,
        cosine,
        sine,
        angle,
        w_nope,
        w_rope,
        w_key,
        w_value,
        latents,
        ropes,
        keys,
        scratch=[
            pltpu.VMEM((kr // LANES + 1, few * heads, LANES), f32),
            pltpu.VMEM((2, few, heads, latent_half[1]), f32),
            pltpu.VMEM(latent_half, bf16),
        ],
    )
    new_latent, new_rope = call(
        functools.partial(fresh_kernel, qr),
        [((n_seq, kr), bf16), ((n_seq, rp), bf16)],
        sums,
        other_sums,
        gain_kv,
        cosine,
        sine,
    )
    self_scores, self_values = call(
        functools.partial(self_kernel, heads, nope),
        [((few, LANES), f32), ((few, heads * vs), f32)],
        latent_new,
        rope_new,
        queries,
        w_value,
    )

    def merge(*parts):
        return call(functools.partial(merge_kernel, heads), [(state, f32)], *parts)[0]

    for masks in kv_rounds:
        part = merge(part, *[swap(part, m | crossing(m)) for m in masks])
    for masks in tp_rounds:
        part = merge(part, *[swap(part, crossing(m), m) for m in masks])
    (part,) = call(
        functools.partial(finish_kernel, heads),
        [((few, heads * vs), f32)],
        part,
        self_scores,
        self_values,
    )
    other = swap(part, 1)
    half = (w_ff_in.shape[1] // 2 // LANES * n_seq + n_seq // 2, LANES)
    resid_mid, keep, give = call(
        middle_kernel,
        [((n_seq, d_dev), f32), (half, f32), (half, f32)],
        part,
        other,
        *kept,
        w_ff_in,
        *w_outs,
        scratch=[pltpu.VMEM((lax.axis_size("tp"), n_seq, w_out_own.shape[0]), bf16)],
    )
    sums = keep + swap(give, 1)
    for masks in kv_rounds:
        sums = paired([sums] + [swap(sums, m | crossing(m)) for m in masks])
    (out,) = call(last_kernel, [((n_seq, d_dev), f32)], sums, swap(sums, 1), w_ff_out)
    for masks in tp_rounds:
        out = paired([out] + [swap(out, 0, m) for m in masks])
    mixed = (resid_mid + out).astype(bf16)
    return (mixed, new_latent, new_rope)


def solution(mesh):
    return sharded(per_device, mesh)


def sharded(step, mesh):
    return jax.shard_map(
        step,
        mesh=mesh,
        in_specs=(
            P(None, "kv"),
            P(),
            P(None, ("kv", "tp"), None),
            P(None, ("kv", "tp"), None),
            P("kv"),
            P("kv", None),
            P("kv", None),
            P("kv", None),
            P(),
            P(),
            P(),
            P(),
            P(),
            P(),
            P("tp", None, "kv"),
            P("kv"),
            P("kv", "tp"),
            P("tp", "kv"),
        ),
        out_specs=(P(None, "kv"), P(), P()),
        check_vma=False,
    )
```
